32 devices in a mesh: ep: 8 (over z, core), tp: 4 (over y, x).
Axes of the slice: x: 2, y: 2, z: 4, core: 2. Of those that a mesh axis runs over, the one named last changes fastest.
Arguments:
- tokens: bfloat16 [1024, 2048], P('ep'), may hold values from -6 to 6
- cotangent: bfloat16 [1024, 2048], P('ep'), may hold values from -6 to 6
- routes: int32 [1024, 2], P('ep'), may hold values from 0 to 7, all different within a row; in each aligned block of 128 rows (0 to 127, 128 to 255, ...) at most 64 rows name the same one
- route_weight: float32 [1024, 2], P('ep'), may hold values from 0.1 to 1
- w_gate: bfloat16 [8, 2048, 1024], P('ep', None, 'tp'), may hold values from -0.1875 to 0.1875
- w_up: bfloat16 [8, 2048, 1024], P('ep', None, 'tp'), may hold values from -0.1875 to 0.1875
- w_down: bfloat16 [8, 1024, 2048], P('ep', 'tp'), may hold values from -0.1875 to 0.1875
Outputs:
- grad_tokens: bfloat16 [1024, 2048], P('ep', 'tp')
- grad_route_weight: float32 [1024, 2], P('ep')
- grad_gate: float32 [8, 2048, 1024], P('ep', None, 'tp')
- grad_up: float32 [8, 2048, 1024], P('ep', None, 'tp')
- grad_down: float32 [8, 1024, 2048], P('ep', 'tp')
The draws below stay inside these ranges and needn't reach their ends.
Inputs may be any that keep to these rules, and one draw needn't show every extreme that they name: `routes`: each row names 2 different experts. In each aligned block of 128 rows (the rows of one index of ep) no expert is named by more than 64 rows, and in every draw some expert is named by exactly 64 rows of some block.
All inputs are finite; a program needn't handle non-finite values.
Results may differ from the reference program's by a relative error of at most 0.023.
Values may be sent and summed in bfloat16 or wider, within the bound.
A program may use at most 64 MiB of HBM per device.

```python
import math
import jax
import jax.numpy as jnp
import numpy as np
from jax import lax

D = 2048
FF = 1024
TOP_K = 2
TOK_DEV = 128
EXPERTS = 8
TOKENS = 1024
CAP = 64
N_EP = 8
N_TP = 4


def strengthened(result, rng, source, target, blocks, factor):
    def block_of(axis_at):
        return (jnp.arange(result.shape[axis_at]) // (result.shape[axis_at] // blocks)).reshape((-1,) + (1,) * (result.ndim - 1 - axis_at))

    near = jax.random.permutation(rng, blocks)[block_of(target)]
    second = (block_of(target) + blocks // 2) % blocks
    return jnp.where((block_of(source) == near) | (block_of(source) == second), factor * result, result)


def levels(rng, shape, cuts, least, top_value):
    def one(dim, shards_of):
        heights = jax.random.uniform(jax.random.fold_in(jax.random.fold_in(rng, 6), dim), (shards_of,), jnp.float32, least / len(cuts), top_value / len(cuts))
        return jnp.repeat(jnp.exp(heights), shape[dim] // shards_of).reshape((-1,) + (1,) * (len(shape) - dim - 1))

    gain = one(*cuts[0])
    for cut in cuts[1:]:
        gain = gain * one(*cut)
    return gain


def routed_block(own_key, own, number, rows, amount, top, bound, slope):
    ranking = jax.random.permutation(own_key, amount)
    packed, common = shares(amount, rows * top, bound, slope, True), shares(amount, rows * top, bound, slope, False)
    places = jnp.arange(amount)

    def named(lengths, rotation):
        used = int((lengths > 0).sum())
        fixed = max(1, used // 4)
        moved = fixed + (places - fixed + rotation * (used - fixed)) % max(1, amount - fixed)
        return jnp.zeros((amount,), jnp.int32).at[ranking[jnp.where(places < fixed, places, moved)]].set(jnp.asarray(lengths, jnp.int32))

    lengths = jnp.where(number % 4 == 0, named(packed, number // 4), named(common, number - number // 4 - 1))
    mixed = jax.random.permutation(jax.random.fold_in(own, 3), amount)
    giver, receiver = mixed[0:amount // 2 * 2:2], mixed[1:amount // 2 * 2:2]
    slack = jnp.minimum(lengths[giver] - 1, bound - lengths[receiver]) // 2
    slack = jnp.where((giver == ranking[0]) | (receiver == ranking[0]) | (lengths[receiver] == 0), 0, jnp.maximum(slack, 0))
    moved = jax.random.randint(jax.random.fold_in(own, 4), (amount // 2,), 0, 1 << 20) % (slack + 1)
    lengths = lengths.at[giver].add(-moved).at[receiver].add(moved)
    members = jnp.searchsorted(jnp.cumsum(lengths), jnp.arange(rows * top), side="right").astype(jnp.int32)
    grid = members.reshape(top, rows).T
    grid = grid[jax.random.permutation(jax.random.fold_in(own, 1), rows)]
    rotation = jax.random.randint(jax.random.fold_in(own, 2), (rows, 1), 0, top)
    return jnp.take_along_axis(grid, (jnp.arange(top)[None, :] + rotation) % top, axis=1)


def shares(number_of, total, bound, lean, full):
    portions = [(1 << 20) // math.isqrt(grade ** lean) + 1 for grade in range(1, number_of + 1)]
    largest = bound if full else min(bound, max(-(-total // number_of), total * portions[0] // sum(portions)))
    least = 1 if total - largest >= number_of - 1 else 0
    holding, surplus = [largest] + [least] * (number_of - 1), total - largest - least * (number_of - 1)
    while surplus > 0:
        free = [i for i in range(1, number_of) if holding[i] < largest] or [i for i in range(1, number_of) if holding[i] < bound]
        pool, budget = sum([portions[i] for i in free]), surplus
        for i in free:
            extra = min(bound - holding[i], max(1, budget * portions[i] // pool), surplus)
            holding[i] = holding[i] + extra
            surplus = surplus - extra
    return np.array(holding)


def scatter_about(stream_key, shape, scale, reach, cuts=(), kind=jnp.bfloat16):
    array = jax.random.normal(stream_key, shape, jnp.float32) * scale
    if len(cuts) > 0:
        array = levels(stream_key, shape, cuts, -0.22, 0.18) * array
    return jnp.clip(array, min=-reach, max=reach).astype(kind)


def gaussian_with(stream_key, shape, spread, reach, shards, heavy, held_as=jnp.bfloat16):
    entries = spread * jax.random.normal(stream_key, shape, jnp.float32)
    if shards:
        entries = entries * levels(stream_key, shape, shards, -0.22, 0.18)
    return jnp.clip(strengthened(entries, jax.random.fold_in(stream_key, 3), *heavy), -reach, reach).astype(held_as)


def setup_inputs(seed: int = 0) -> dict:
    key_list = jax.random.split(jax.random.key(seed), 8)
    tokens = scatter_about(key_list[0], (TOKENS, D), 1.0, 6.0, ((0, 8),))
    cotangent = scatter_about(key_list[1], (TOKENS, D), 1.0, 6.0, ((0, 8),))
    routes_keys = jax.random.split(jax.random.fold_in(key_list[2], 1), TOKENS // TOK_DEV)
    routes_turns = jax.random.permutation(jax.random.fold_in(key_list[2], 3), TOKENS // TOK_DEV)
    routes = jax.vmap(lambda own, number: routed_block(jax.random.fold_in(key_list[2], 2), own, number, TOK_DEV, EXPERTS, TOP_K, CAP, 2))(routes_keys, routes_turns).reshape((TOKENS, TOP_K))
    route_weight = jnp.clip(0.1 + 0.9 * jax.random.uniform(key_list[3], (TOKENS, TOP_K), jnp.float32) ** levels(key_list[3], (TOKENS, TOP_K), ((0, 8),), -0.2, 0.2), 0.1, 1.0)
    w_gate = gaussian_with(key_list[4], (EXPERTS, D, FF), D ** -0.5, 0.1875, ((0, 8), (2, 4)), (2, 1, 4, 2.0))
    w_up = gaussian_with(key_list[5], (EXPERTS, D, FF), D ** -0.5, 0.1875, ((0, 8), (2, 4)), (2, 1, 4, 2.0))
    w_down = scatter_about(key_list[6], (EXPERTS, FF, D), FF ** -0.5, 0.1875, ((0, 8), (1, 4)))
    return {"tokens": tokens, "cotangent": cotangent, "routes": routes, "route_weight": route_weight, "w_gate": w_gate, "w_up": w_up, "w_down": w_down}


def slot_index(block_routes, experts, capacity):
    flat_ids = block_routes.reshape(-1)
    onehot = (flat_ids[:, None] == jnp.arange(experts, dtype=jnp.int32)[None, :]).astype(jnp.int32)
    earlier = jnp.cumsum(onehot, axis=0) - onehot
    return flat_ids * capacity + jnp.sum(earlier * onehot, axis=1)


def expert_grads(inputs):
    rows_x, rows_dy, rows_w, gate_w, up_w, down_w = inputs
    f32 = jnp.float32
    n_rows, model_width = rows_x.shape
    gate_pre = jnp.dot(rows_x, gate_w, preferred_element_type=f32)
    up_pre = jnp.dot(rows_x, up_w, preferred_element_type=f32)
    gate_sig = jax.nn.sigmoid(gate_pre)
    act_full = gate_pre * gate_sig * up_pre
    act = act_full.astype(jnp.bfloat16)
    back_hidden = jnp.dot(rows_dy, down_w.T, preferred_element_type=f32)
    weighted_cot = (rows_w[:, None] * rows_dy.astype(f32)).astype(jnp.bfloat16)
    d_hidden = rows_w[:, None] * back_hidden
    d_gate = (d_hidden * up_pre * gate_sig * (1.0 + gate_pre * (1.0 - gate_sig))).astype(jnp.bfloat16)
    d_up = (d_hidden * gate_pre * gate_sig).astype(jnp.bfloat16)
    gate_grad = jnp.sum(act_full * back_hidden, axis=1)
    pieces = jnp.einsum('rjf,djf->jrd', d_gate.astype(f32).reshape(n_rows, N_TP, -1),
                        gate_w.astype(f32).reshape(model_width, N_TP, -1), precision=lax.Precision.HIGHEST)
    pieces = pieces + jnp.einsum('rjf,djf->jrd', d_up.astype(f32).reshape(n_rows, N_TP, -1),
                                 up_w.astype(f32).reshape(model_width, N_TP, -1), precision=lax.Precision.HIGHEST)
    rounded = lax.optimization_barrier(pieces.astype(jnp.bfloat16))
    route_grad = jnp.sum(rounded.astype(f32), axis=0).astype(jnp.bfloat16)
    grad_gate_e = jnp.dot(rows_x.T, d_gate, preferred_element_type=f32)
    grad_up_e = jnp.dot(rows_x.T, d_up, preferred_element_type=f32)
    grad_down_e = jnp.dot(act.T, weighted_cot, preferred_element_type=f32)
    return route_grad, gate_grad, grad_gate_e, grad_up_e, grad_down_e


def reference(tokens, cotangent, routes, route_weight, w_gate, w_up, w_down):
    f32 = jnp.float32
    blocks = routes.reshape(N_EP, TOK_DEV, TOP_K)
    slot_ids = jax.vmap(lambda block: slot_index(block, EXPERTS, CAP))(blocks)
    expert_ids = blocks.reshape(N_EP, TOK_DEV * TOP_K)
    positions = slot_ids - expert_ids * CAP
    sources = jnp.arange(N_EP, dtype=jnp.int32)[:, None]
    rows_x = jnp.repeat(tokens.reshape(N_EP, TOK_DEV, D), TOP_K, axis=1)
    rows_dy = jnp.repeat(cotangent.reshape(N_EP, TOK_DEV, D), TOP_K, axis=1)
    rows_w = route_weight.reshape(N_EP, TOK_DEV * TOP_K)
    buf_x = jnp.zeros((EXPERTS, N_EP, CAP, D), jnp.bfloat16).at[expert_ids, sources, positions].set(rows_x)
    buf_dy = jnp.zeros((EXPERTS, N_EP, CAP, D), jnp.bfloat16).at[expert_ids, sources, positions].set(rows_dy)
    buf_w = jnp.zeros((EXPERTS, N_EP, CAP), f32).at[expert_ids, sources, positions].set(rows_w)
    recv_rows = N_EP * CAP
    outs = lax.map(expert_grads, (buf_x.reshape(EXPERTS, recv_rows, D), buf_dy.reshape(EXPERTS, recv_rows, D),
                                  buf_w.reshape(EXPERTS, recv_rows), w_gate, w_up, w_down))
    route_grad, gate_grad, grad_gate, grad_up, grad_down = outs
    back_index = sources * CAP + positions
    picked = route_grad[expert_ids, back_index].astype(f32).reshape(TOKENS, TOP_K, D)
    grad_tokens = jnp.sum(picked, axis=1).astype(jnp.bfloat16)
    grad_route_weight = gate_grad[expert_ids, back_index].reshape(TOKENS, TOP_K)
    return grad_tokens, grad_route_weight, grad_gate, grad_up, grad_down
```

```python
import functools

import jax
import jax.numpy as jnp
from jax import lax
from jax.experimental import pallas as pl
from jax.experimental.pallas import tpu as pltpu
from jax.sharding import PartitionSpec as P


def slot_index(block_routes, experts, capacity):
    flat_ids = block_routes.reshape(-1)
    onehot = (flat_ids[:, None] == jnp.arange(experts, dtype=jnp.int32)[None, :]).astype(jnp.int32)
    earlier = jnp.cumsum(onehot, axis=0) - onehot
    return flat_ids * capacity + jnp.sum(earlier * onehot, axis=1)


def slotted(tokens, cotangent, routes, route_weight, w_gate, w_up, w_down):
    f32 = jnp.float32
    tok_rows, model_width = tokens.shape
    choices_row = routes.shape[1]
    experts = lax.axis_size("ep")
    capacity = 2 * tok_rows * choices_row // experts
    recv_rows = experts * capacity
    slot_ids = slot_index(routes, experts, capacity)
    send_w = jnp.zeros((recv_rows,), f32).at[slot_ids].set(route_weight.reshape(-1))
    send_x = (
        jnp.zeros((recv_rows, model_width), jnp.bfloat16)
        .at[slot_ids]
        .set(jnp.repeat(tokens, choices_row, axis=0))
    )
    send_dy = (
        jnp.zeros((recv_rows, model_width), jnp.bfloat16)
        .at[slot_ids]
        .set(jnp.repeat(cotangent, choices_row, axis=0))
    )
    got_x = lax.all_to_all(
        send_x.reshape(experts, capacity, model_width),
        "ep",
        split_axis=0,
        concat_axis=0,
        tiled=True,
    )
    got_dy, got_w = (
        lax.all_to_all(
            send_dy.reshape(experts, capacity, model_width),
            "ep",
            split_axis=0,
            concat_axis=0,
            tiled=True,
        ),
        lax.all_to_all(
            send_w.reshape(experts, capacity, 1).astype(jnp.bfloat16),
            "ep",
            split_axis=0,
            concat_axis=0,
            tiled=True,
        ).astype(jnp.float32),
    )
    rows_x = got_x.reshape(recv_rows, model_width)
    rows_dy = got_dy.reshape(recv_rows, model_width)
    rows_w = got_w.reshape(recv_rows)
    gate_w = w_gate[0]
    up_w = w_up[0]
    down_w = w_down[0]
    gate_pre = jnp.dot(rows_x, gate_w, preferred_element_type=f32)
    up_pre = jnp.dot(rows_x, up_w, preferred_element_type=f32)
    gate_sig = jax.nn.sigmoid(gate_pre)
    act_full = gate_pre * gate_sig * up_pre
    act = act_full.astype(jnp.bfloat16)
    back_hidden = jnp.einsum("rd,fd->rf", rows_dy, down_w, preferred_element_type=f32)
    weighted_cot = (rows_w[:, None] * rows_dy.astype(f32)).astype(jnp.bfloat16)
    d_hidden = rows_w[:, None] * back_hidden
    d_gate = (d_hidden * up_pre * gate_sig * (1.0 + gate_pre * (1.0 - gate_sig))).astype(
        jnp.bfloat16
    )
    d_up = (d_hidden * gate_pre * gate_sig).astype(jnp.bfloat16)
    gate_part = jnp.sum(act_full * back_hidden, axis=1)
    token_part = jnp.einsum("rf,df->rd", d_gate, gate_w, preferred_element_type=f32)
    token_part = token_part + jnp.einsum("rf,df->rd", d_up, up_w, preferred_element_type=f32)
    grad_gate = jnp.einsum("rd,rf->df", rows_x, d_gate, preferred_element_type=f32)[None]
    grad_up = jnp.einsum("rd,rf->df", rows_x, d_up, preferred_element_type=f32)[None]
    grad_down = jnp.einsum("rf,rd->fd", act, weighted_cot, preferred_element_type=f32)[None]
    rounded_part = token_part.astype(jnp.bfloat16).astype(f32)
    shares = lax.psum_scatter(
        rounded_part.astype(jnp.bfloat16), "tp", scatter_dimension=1, tiled=True
    )
    gate_total = lax.psum(gate_part, "tp")
    back_x, back_gate = (
        lax.all_to_all(
            shares.reshape(experts, capacity, -1), "ep", split_axis=0, concat_axis=0, tiled=True
        ),
        lax.all_to_all(
            gate_total.reshape(experts, capacity).astype(jnp.bfloat16),
            "ep",
            split_axis=0,
            concat_axis=0,
            tiled=True,
        ).astype(jnp.float32),
    )
    picked = back_x.reshape(recv_rows, -1)[slot_ids].astype(f32).reshape(tok_rows, choices_row, -1)
    grad_route_weight = back_gate.reshape(recv_rows)[slot_ids].reshape(tok_rows, choices_row)
    grad_tokens = jnp.sum(picked, axis=1).astype(jnp.bfloat16)
    return (grad_tokens, grad_route_weight, grad_gate, grad_up, grad_down)


def kernel(ep, tp, tokens, cotangent, routes, route_weight, w_gate, w_up, w_down,
           result, out_home, g_gate, g_up, g_down,
           full, gate_v, up_v, down_v, weights, part, other, top, bottom,
           in_top, in_bottom, last_top, last_bottom, share, arrived,
           d_gate, d_up, act_w, table, score, scores, total, home,
           local, sent, got):
    f32, bf16 = jnp.float32, jnp.bfloat16
    rows, width = tokens.shape
    cols = width // tp
    half = rows // 2
    nz = ep // 2
    e, t = lax.axis_index("ep"), lax.axis_index("tp")
    z, c = e // 2, lax.rem(e, 2)
    y, x = t // 2, lax.rem(t, 2)
    side = z * 2 + 1 - c
    tx, ty = y * 2 + 1 - x, (1 - y) * 2 + x
    td = (1 - y) * 2 + 1 - x
    slots, started, locals_ = {}, [], []

    def slot(*name):
        return got.at[slots.setdefault(name, len(slots))]

    def push(src, dst, name, to_e, to_t):
        copy = pltpu.make_async_remote_copy(
            src_ref=src, dst_ref=dst, send_sem=sent.at[len(started)], recv_sem=slot(*name),
            device_id={"ep": to_e, "tp": to_t}, device_id_type=pl.DeviceIdType.MESH)
        copy.start()
        started.append(copy)

    def landed(dst, *name):
        pltpu.make_async_remote_copy(
            src_ref=dst, dst_ref=dst, send_sem=sent.at[0], recv_sem=slot(*name),
            device_id={"ep": side, "tp": t}, device_id_type=pl.DeviceIdType.MESH).wait_recv()

    def bring(src, dst):
        copy = pltpu.make_async_copy(src, dst, local.at[len(locals_)])
        copy.start()
        locals_.append(copy)
        return copy

    own = [bring(ref.at[:, pl.ds(q * cols, cols)], full.at[e, a, q])
           for a, ref in enumerate((tokens, cotangent)) for q in range(tp)]
    loads = [bring(w_gate.at[0], gate_v), bring(w_up.at[0], up_v), bring(w_down.at[0], down_v)]
    named = lax.broadcasted_iota(jnp.int32, (ep, rows), 0)
    hits = [named == routes[pl.ds(k, 1), :] for k in range(routes.shape[0])]
    table[...] = sum(jnp.where(hit, route_weight[pl.ds(k, 1), :], 0.0) for k, hit in enumerate(hits))
    weights[e] = table[...]

    barrier = pltpu.get_barrier_semaphore()
    for k in range(1, ep):
        pl.semaphore_signal(barrier, inc=1, device_id={"ep": lax.rem(e + k, ep), "tp": t},
                            device_id_type=pl.DeviceIdType.MESH)
    for k in range(1, tp):
        pl.semaphore_signal(barrier, inc=1, device_id={"ep": e, "tp": lax.rem(t + k, tp)},
                            device_id_type=pl.DeviceIdType.MESH)
    pl.semaphore_wait(barrier, ep + tp - 2)

    edge = jnp.minimum(z, nz - 1 - z)

    def back(i):
        near = z + (i + 1) // 2 * (1 - i % 2 * 2)
        away = jnp.where(z < nz - 1 - z, z + i - edge, z - i + edge)
        return jnp.where(i <= 2 * edge, near, away) if i else z

    relays = []

    def along(piece, from_z, a, go, to_z):
        copy = pltpu.make_async_remote_copy(
            src_ref=piece, dst_ref=piece, send_sem=sent.at[20 * nz + len(relays)],
            recv_sem=got.at[20 * nz + from_z * 2 + a],
            device_id={"ep": to_z * 2 + c, "tp": t}, device_id_type=pl.DeviceIdType.MESH)
        pl.when(go)(copy.start)
        relays.append((go, copy))

    for copy in own:
        copy.wait()
    for a in range(2):
        along(full.at[e, a, t], z, a, z < nz - 1, jnp.minimum(z + 1, nz - 1))
        along(full.at[e, a, t], z, a, z > 0, jnp.maximum(z - 1, 0))
    for a in range(2):
        push(full.at[e, a], full.at[e, a], ("side", 0, a), side, t)
    for k in range(1, ep):
        push(table, weights.at[e], ("w", k), lax.rem(e + k, ep), t)

    def spread(dz):
        s = back(dz) * 2 + c
        for a in range(2):
            piece = full.at[s, a, t]
            pltpu.make_async_remote_copy(
                src_ref=piece, dst_ref=piece, send_sem=sent.at[0],
                recv_sem=got.at[20 * nz + back(dz) * 2 + a],
                device_id={"ep": side, "tp": t}, device_id_type=pl.DeviceIdType.MESH).wait_recv()
            below = back(dz) < z
            go = jnp.where(below, z < nz - 1, z > 0)
            onward = jnp.where(below, jnp.minimum(z + 1, nz - 1), jnp.maximum(z - 1, 0))
            along(piece, back(dz), a, go, onward)
            push(piece, piece, ("x", dz, a), e, tx)
            push(piece, piece, ("y", dz, a), e, ty)

    def relay(dz):
        s = back(dz) * 2 + c
        piece = full.at[s, 0, ty]
        landed(piece, "y", dz, 0)
        push(piece, piece, ("d", dz, 0), e, tx)
        piece = full.at[s, 1, tx]
        landed(piece, "x", dz, 1)
        push(piece, piece, ("d", dz, 1), e, ty)

    def hand(dz):
        s = back(dz) * 2 + c
        landed(full.at[s, 0, tx], "x", dz, 0)
        landed(full.at[s, 0, td], "d", dz, 0)
        push(full.at[s, 0], full.at[s, 0], ("side", dz, 0), side, t)
        landed(full.at[s, 1, ty], "y", dz, 1)
        landed(full.at[s, 1, td], "d", dz, 1)
        push(full.at[s, 1], full.at[s, 1], ("side", dz, 1), side, t)

    def nt(a, b):
        return lax.dot_general(a, b, (((1,), (1,)), ((), ())), preferred_element_type=f32)

    def tn(a, b):
        return lax.dot_general(a, b, (((0,), (0,)), ((), ())), preferred_element_type=f32)

    def column(block):
        mine = lax.broadcasted_iota(jnp.int32, (ep, rows), 0) == e
        row = jnp.sum(jnp.where(mine, weights[block], 0.0), axis=0, keepdims=True)
        return jnp.transpose(jnp.broadcast_to(row, (rows, rows)))[:, :1]

    def compute(dz):
        b = back(dz) * 2
        for a in range(2):
            landed(full.at[back(dz) * 2 + 1 - c, a], "side", dz, a)
        g = u = bk = None
        for q in range(tp):
            span = pl.ds(q * cols, cols)
            xs = jnp.concatenate([full[b, 0, q], full[b + 1, 0, q]], axis=0)
            dy = jnp.concatenate([full[b, 1, q], full[b + 1, 1, q]], axis=0)
            g_q = jnp.dot(xs, gate_v[span, :], preferred_element_type=f32)
            u_q = jnp.dot(xs, up_v[span, :], preferred_element_type=f32)
            b_q = nt(dy, down_v[:, span])
            g, u, bk = (g_q, u_q, b_q) if q == 0 else (g + g_q, u + u_q, bk + b_q)
        w = jnp.concatenate([column(b), column(b + 1)], axis=0)
        sig = jax.nn.sigmoid(g)
        silu = g * sig
        act = silu * u
        d_h = w * bk
        dg = (d_h * u * sig * (1.0 + g * (1.0 - sig))).astype(bf16)
        du = (d_h * silu).astype(bf16)
        aw = (w * act).astype(bf16)
        sums = jnp.sum(act * bk, axis=1, keepdims=True)
        for i in range(2):
            cut = slice(i * rows, (i + 1) * rows)
            d_gate[b + i] = dg[cut]
            d_up[b + i] = du[cut]
            act_w[b + i] = aw[cut]
            score[b + i] = jnp.transpose(jnp.broadcast_to(sums[cut], (rows, rows)))[:8]
        for q in range(tp):
            span = pl.ds(q * cols, cols)
            piece = (nt(dg, gate_v[span, :]) + nt(du, up_v[span, :])).astype(bf16)
            part[b, q] = piece[:rows]
            part[b + 1, q] = piece[rows:]
        push(part.at[back(dz) * 2 + 1 - c], other.at[dz], ("pair", dz), side, t)

    for copy in loads:
        copy.wait()
    for k in range(1, ep):
        landed(weights.at[lax.rem(e - k + ep, ep)], "w", k)

    def add(*terms):
        value = terms[0].astype(f32)
        for term in terms[1:]:
            value = value + term.astype(f32)
        return value

    def first(dz):
        s = back(dz) * 2 + c
        landed(other.at[dz], "pair", dz)
        for r, q in enumerate((t, ty, tx, td)):
            top[dz, r] = add(part[s, q, :half], other[dz, q, :half]).astype(bf16)
        push(top.at[dz, pl.ds(2, 2)], in_top.at[dz], ("top", dz), e, tx)
        for r, q in enumerate((t, tx, ty, td)):
            bottom[dz, r] = add(part[s, q, half:], other[dz, q, half:]).astype(bf16)
        push(bottom.at[dz, pl.ds(2, 2)], in_bottom.at[dz], ("bottom", dz), e, ty)

    def second(dz):
        landed(in_top.at[dz], "top", dz)
        top[dz, 1] = add(top[dz, 1], in_top[dz, 1]).astype(bf16)
        push(top.at[dz, 1], last_top.at[dz], ("last_top", dz), e, ty)
        landed(in_bottom.at[dz], "bottom", dz)
        bottom[dz, 1] = add(bottom[dz, 1], in_bottom[dz, 1]).astype(bf16)
        push(bottom.at[dz, 1], last_bottom.at[dz], ("last_bottom", dz), e, tx)

    def third(dz):
        landed(last_top.at[dz], "last_top", dz)
        landed(last_bottom.at[dz], "last_bottom", dz)
        upper = add(top[dz, 0], in_top[dz, 0], last_top[dz])
        lower = add(bottom[dz, 0], in_bottom[dz, 0], last_bottom[dz])
        if dz:
            share[dz - 1, :half] = upper.astype(bf16)
            share[dz - 1, half:] = lower.astype(bf16)
            copy = pltpu.make_async_remote_copy(
                src_ref=share.at[dz - 1], dst_ref=arrived.at[z], send_sem=sent.at[len(started)],
                recv_sem=got.at[22 * nz + z], device_id={"ep": back(dz) * 2 + c, "tp": t},
                device_id_type=pl.DeviceIdType.MESH)
            copy.start()
            started.append(copy)
        return upper, lower

    def by_width(out, ref):
        right = ref[...].reshape(ep * rows, ref.shape[2])
        for q in range(tp):
            out[0, pl.ds(q * cols, cols), :] = tn(full[:, 0, q].reshape(ep * rows, cols), right)

    spread(1)
    compute(0)
    if nz > 2:
        spread(2)
    for dz in range(1, nz):
        relay(dz)
        if dz + 2 < nz:
            spread(dz + 2)
        if dz > 1:
            second(dz - 2)
        first(dz - 1)
        hand(dz)
        compute(dz)
    for k in range(1, tp):
        push(score, scores.at[t], ("score", k), e, lax.rem(t + k, tp))
    scores[t] = score[...]
    for dz in range(1, nz - 2):
        third(dz)
    second(nz - 2)
    first(nz - 1)
    by_width(g_gate, d_gate)
    for dz in range(max(1, nz - 2), nz - 1):
        third(dz)
    second(nz - 1)
    for k in range(1, tp):
        landed(scores.at[lax.rem(t - k + tp, tp)], "score", k)
    total[...] = add(*[scores[j] for j in range(tp)])
    for k in range(1, ep):
        to = lax.rem(e + k, ep)
        push(total.at[to], home.at[e], ("home", k), to, t)
    home[e] = total[e]
    by_width(g_up, d_up)
    third(nz - 1)
    left = act_w[...].reshape(ep * rows, act_w.shape[2])
    for q in range(tp):
        g_down[0, :, pl.ds(q * cols, cols)] = tn(left, full[:, 1, q].reshape(ep * rows, cols))
    upper, lower = third(0)
    for k in range(1, nz):
        j = lax.rem(z + k, nz)
        pltpu.make_async_remote_copy(
            src_ref=arrived.at[j], dst_ref=arrived.at[j], send_sem=sent.at[0],
            recv_sem=got.at[22 * nz + j], device_id={"ep": side, "tp": t},
            device_id_type=pl.DeviceIdType.MESH).wait_recv()
        upper = upper + arrived[j, :half].astype(f32)
        lower = lower + arrived[j, half:].astype(f32)
    result[:half] = upper.astype(bf16)
    result[half:] = lower.astype(bf16)
    for k in range(1, ep):
        landed(home.at[lax.rem(e - k + ep, ep)], "home", k)
    back_home = jnp.concatenate([home[j, :1] for j in range(ep)], axis=0)
    for k, hit in enumerate(hits):
        out_home[pl.ds(k, 1), :] = jnp.sum(jnp.where(hit, back_home, 0.0), axis=0, keepdims=True)
    assert len(started) <= 20 * nz and len(slots) <= 20 * nz and len(relays) <= 4 * nz
    for copy in started:
        copy.wait_send()
    for go, copy in relays:
        pl.when(go)(copy.wait_send)


def deliver(*refs):
    half = (len(refs) - 1) // 2
    copies = [pltpu.make_async_copy(src, dst, refs[-1].at[i])
              for i, (src, dst) in enumerate(zip(refs[:half], refs[half:-1]))]
    for copy in copies:
        copy.start()
    for copy in copies:
        copy.wait()


def dense(tokens, cotangent, routes, route_weight, w_gate, w_up, w_down):
    f32, bf16 = jnp.float32, jnp.bfloat16
    rows, width = tokens.shape
    ep, tp = lax.axis_size("ep"), lax.axis_size("tp")
    cols, half, nz, hidden = width // tp, rows // 2, ep // 2, w_gate.shape[2]
    anywhere, near = pl.BlockSpec(memory_space=pltpu.HBM), pl.BlockSpec(memory_space=pltpu.VMEM)

    def held(space, *arrays):
        return [pltpu.with_memory_space_constraint(x, space) for x in arrays]

    shapes = ((rows, cols), bf16), (routes.T.shape, f32), (w_gate.shape, f32), (w_up.shape, f32), (w_down.shape, f32)
    parts = pl.pallas_call(
        functools.partial(kernel, ep, tp),
        out_shape=tuple(pltpu.VMEM(*shape) for shape in shapes),
        in_specs=[anywhere, anywhere, near, near, anywhere, anywhere, anywhere],
        out_specs=(near,) * 5,
        scratch_shapes=[
            pltpu.VMEM((ep, 2, tp, rows, cols), bf16),
            pltpu.VMEM((width, hidden), bf16),
            pltpu.VMEM((width, hidden), bf16),
            pltpu.VMEM((hidden, width), bf16),
            pltpu.VMEM((ep, ep, rows), f32),
            pltpu.VMEM((ep, tp, rows, cols), bf16),
            pltpu.VMEM((nz, tp, rows, cols), bf16),
            pltpu.VMEM((nz, 4, half, cols), bf16),
            pltpu.VMEM((nz, 4, half, cols), bf16),
            pltpu.VMEM((nz, 2, half, cols), bf16),
            pltpu.VMEM((nz, 2, half, cols), bf16),
            pltpu.VMEM((nz, half, cols), bf16),
            pltpu.VMEM((nz, half, cols), bf16),
            pltpu.VMEM((nz - 1, rows, cols), bf16),
            pltpu.VMEM((nz, rows, cols), bf16),
            pltpu.VMEM((ep, rows, hidden), bf16),
            pltpu.VMEM((ep, rows, hidden), bf16),
            pltpu.VMEM((ep, rows, hidden), bf16),
            pltpu.VMEM((ep, rows), f32),
            pltpu.VMEM((ep, 8, rows), f32),
            pltpu.VMEM((tp, ep, 8, rows), f32),
            pltpu.VMEM((ep, 8, rows), f32),
            pltpu.VMEM((ep, 8, rows), f32),
            pltpu.SemaphoreType.DMA((16 + 2 * tp,)),
            pltpu.SemaphoreType.DMA((24 * nz,)),
            pltpu.SemaphoreType.DMA((24 * nz,)),
        ],
        compiler_params=pltpu.CompilerParams(
            collective_id=0, has_side_effects=True, vmem_limit_bytes=50 * 1024 * 1024),
    )(*held(pltpu.HBM, tokens, cotangent), routes.T, route_weight.T,
      *held(pltpu.HBM, w_gate, w_up, w_down))
    grad_tokens, grw, *grads = pl.pallas_call(
        deliver,
        out_shape=tuple(jax.ShapeDtypeStruct(*shape) for shape in shapes),
        in_specs=[near] * 5,
        out_specs=(anywhere,) * 5,
        scratch_shapes=[pltpu.SemaphoreType.DMA((5,))],
        compiler_params=pltpu.CompilerParams(vmem_limit_bytes=1 << 20),
    )(*held(pltpu.VMEM, *parts))
    return grad_tokens, grw.T, *grads


def on_device(*args):
    rows, width = args[0].shape
    ep, tp = lax.axis_size("ep"), lax.axis_size("tp")
    fits = tp == 4 and ep % 2 == 0 and rows % 128 == 0 and 4 * rows * width * ep <= 1 << 24
    return (dense if fits else slotted)(*args)


def solution(mesh):
    return jax.shard_map(
        on_device,
        mesh=mesh,
        in_specs=(
            P("ep", None),
            P("ep", None),
            P("ep", None),
            P("ep", None),
            P("ep", None, "tp"),
            P("ep", None, "tp"),
            P("ep", "tp", None),
        ),
        out_specs=(
            P("ep", "tp"),
            P("ep", None),
            P("ep", None, "tp"),
            P("ep", None, "tp"),
            P("ep", "tp", None),
        ),
        check_vma=False,
    )
```

```python
import functools

import jax
import jax.numpy as jnp
from jax import lax
from jax.experimental import pallas as pl
from jax.experimental.pallas import tpu as pltpu
from jax.sharding import PartitionSpec as P


def slot_index(block_routes, experts, capacity):
    flat_ids = block_routes.reshape(-1)
    onehot = (flat_ids[:, None] == jnp.arange(experts, dtype=jnp.int32)[None, :]).astype(jnp.int32)
    earlier = jnp.cumsum(onehot, axis=0) - onehot
    return flat_ids * capacity + jnp.sum(earlier * onehot, axis=1)


def slotted(tokens, cotangent, routes, route_weight, w_gate, w_up, w_down):
    f32 = jnp.float32
    tok_rows, model_width = tokens.shape
    choices_row = routes.shape[1]
    experts = lax.axis_size("ep")
    capacity = 2 * tok_rows * choices_row // experts
    recv_rows = experts * capacity
    slot_ids = slot_index(routes, experts, capacity)
    send_w = jnp.zeros((recv_rows,), f32).at[slot_ids].set(route_weight.reshape(-1))
    send_x = (
        jnp.zeros((recv_rows, model_width), jnp.bfloat16)
        .at[slot_ids]
        .set(jnp.repeat(tokens, choices_row, axis=0))
    )
    send_dy = (
        jnp.zeros((recv_rows, model_width), jnp.bfloat16)
        .at[slot_ids]
        .set(jnp.repeat(cotangent, choices_row, axis=0))
    )
    got_x = lax.all_to_all(
        send_x.reshape(experts, capacity, model_width),
        "ep",
        split_axis=0,
        concat_axis=0,
        tiled=True,
    )
    got_dy, got_w = (
        lax.all_to_all(
            send_dy.reshape(experts, capacity, model_width),
            "ep",
            split_axis=0,
            concat_axis=0,
            tiled=True,
        ),
        lax.all_to_all(
            send_w.reshape(experts, capacity, 1).astype(jnp.bfloat16),
            "ep",
            split_axis=0,
            concat_axis=0,
            tiled=True,
        ).astype(jnp.float32),
    )
    rows_x = got_x.reshape(recv_rows, model_width)
    rows_dy = got_dy.reshape(recv_rows, model_width)
    rows_w = got_w.reshape(recv_rows)
    gate_w = w_gate[0]
    up_w = w_up[0]
    down_w = w_down[0]
    gate_pre = jnp.dot(rows_x, gate_w, preferred_element_type=f32)
    up_pre = jnp.dot(rows_x, up_w, preferred_element_type=f32)
    gate_sig = jax.nn.sigmoid(gate_pre)
    act_full = gate_pre * gate_sig * up_pre
    act = act_full.astype(jnp.bfloat16)
    back_hidden = jnp.einsum("rd,fd->rf", rows_dy, down_w, preferred_element_type=f32)
    weighted_cot = (rows_w[:, None] * rows_dy.astype(f32)).astype(jnp.bfloat16)
    d_hidden = rows_w[:, None] * back_hidden
    d_gate = (d_hidden * up_pre * gate_sig * (1.0 + gate_pre * (1.0 - gate_sig))).astype(
        jnp.bfloat16
    )
    d_up = (d_hidden * gate_pre * gate_sig).astype(jnp.bfloat16)
    gate_part = jnp.sum(act_full * back_hidden, axis=1)
    token_part = jnp.einsum("rf,df->rd", d_gate, gate_w, preferred_element_type=f32)
    token_part = token_part + jnp.einsum("rf,df->rd", d_up, up_w, preferred_element_type=f32)
    grad_gate = jnp.einsum("rd,rf->df", rows_x, d_gate, preferred_element_type=f32)[None]
    grad_up = jnp.einsum("rd,rf->df", rows_x, d_up, preferred_element_type=f32)[None]
    grad_down = jnp.einsum("rf,rd->fd", act, weighted_cot, preferred_element_type=f32)[None]
    rounded_part = token_part.astype(jnp.bfloat16).astype(f32)
    shares = lax.psum_scatter(
        rounded_part.astype(jnp.bfloat16), "tp", scatter_dimension=1, tiled=True
    )
    gate_total = lax.psum(gate_part, "tp")
    back_x, back_gate = (
        lax.all_to_all(
            shares.reshape(experts, capacity, -1), "ep", split_axis=0, concat_axis=0, tiled=True
        ),
        lax.all_to_all(
            gate_total.reshape(experts, capacity).astype(jnp.bfloat16),
            "ep",
            split_axis=0,
            concat_axis=0,
            tiled=True,
        ).astype(jnp.float32),
    )
    picked = back_x.reshape(recv_rows, -1)[slot_ids].astype(f32).reshape(tok_rows, choices_row, -1)
    grad_route_weight = back_gate.reshape(recv_rows)[slot_ids].reshape(tok_rows, choices_row)
    grad_tokens = jnp.sum(picked, axis=1).astype(jnp.bfloat16)
    return (grad_tokens, grad_route_weight, grad_gate, grad_up, grad_down)


def kernel(ep, tp, tokens, cotangent, routes, route_weight, w_gate, w_up, w_down,
           result, out_home, g_gate, g_up, g_down,
           full, gate_v, up_v, down_v, weights, part, other, top, bottom,
           in_top, in_bottom, last_top, last_bottom, share, arrived,
           d_gate, d_up, act_w, score, score_rows, scores, total, home,
           local, sent, got):
    f32, bf16 = jnp.float32, jnp.bfloat16
    rows, width = tokens.shape
    cols = width // tp
    half = rows // 2
    nz = ep // 2
    e, t = lax.axis_index("ep"), lax.axis_index("tp")
    z, c = e // 2, lax.rem(e, 2)
    y, x = t // 2, lax.rem(t, 2)
    side = z * 2 + 1 - c
    tx, ty = y * 2 + 1 - x, (1 - y) * 2 + x
    td = (1 - y) * 2 + 1 - x
    onward = jnp.where(z < nz // 2, 1, -1)
    middle = jnp.logical_and(z > 0, z < nz - 1)
    outer = jnp.logical_not(middle)
    lead = jnp.where(middle, onward, 0)
    back = [z, z + onward - 2 * lead, z + 2 * onward, z + 3 * onward - 2 * lead]
    behind, ahead = z + onward - 2 * lead, z + onward
    names = {}
    groups = {"pair": 0, "plane": 1, "side": 2, "own": 3, "halves": 4, "quarters": 5, "home": 6, "small": 7,
              "relay": 8, "relay_w": 9}

    def scope(name):
        return jax.named_scope(name)

    def slot(name, count=1):
        if name not in names:
            names[name] = sum(n for _, n in names.values()), count
        return names[name][0]

    def plan(group, src, dst, slot_at, to_e, to_t):
        return pltpu.make_async_remote_copy(
            src_ref=src, dst_ref=dst, send_sem=sent.at[groups[group]], recv_sem=got.at[slot_at],
            device_id={"ep": to_e, "tp": to_t}, device_id_type=pl.DeviceIdType.MESH)

    def push(*args):
        plan(*args).start()

    def drained(group, ref):
        pltpu.make_async_remote_copy(
            src_ref=ref, dst_ref=ref, send_sem=sent.at[groups[group]], recv_sem=got.at[0],
            device_id={"ep": side, "tp": t}, device_id_type=pl.DeviceIdType.MESH).wait_send()

    def landing(dst, slot_at):
        return pltpu.make_async_remote_copy(
            src_ref=dst, dst_ref=dst, send_sem=sent.at[0], recv_sem=got.at[slot_at],
            device_id={"ep": side, "tp": t}, device_id_type=pl.DeviceIdType.MESH)

    def landed(dst, slot_at, label="w"):
        with scope(label):
            landing(dst, slot_at).wait_recv()

    own = [pltpu.make_async_copy(ref.at[:, pl.ds(q * cols, cols)], full.at[e, a, q], local.at[0])
           for a, ref in enumerate((tokens, cotangent)) for q in range(tp)]
    loads = [pltpu.make_async_copy(src.at[0], dst, local.at[1 + i])
             for i, (src, dst) in enumerate(((w_gate, gate_v), (w_up, up_v), (w_down, down_v)))]
    for copy in own + loads:
        copy.start()
    slot("along", 4 * nz), slot("x", 2 * nz - 2), slot("y", 2 * nz - 2), slot("dx", nz - 1), slot("dy", nz - 1)
    slot("side", nz), slot("side_w", nz), slot("pair", 3 * nz), slot("top", nz), slot("bottom", nz)
    slot("last_top", nz), slot("last_bottom", nz), slot("share"), slot("score"), slot("home")

    barrier = pltpu.get_barrier_semaphore()

    def greet(to_e, to_t):
        pl.semaphore_signal(barrier, inc=1, device_id={"ep": to_e, "tp": to_t},
                            device_id_type=pl.DeviceIdType.MESH)

    greet(side, t)
    greet(e, tx)
    greet(e, ty)
    greet(ahead * 2 + c, t)
    pl.when(middle)(lambda: greet(behind * 2 + c, t))

    named = lax.broadcasted_iota(jnp.int32, (ep, rows), 0)
    hits = [named == routes[pl.ds(k, 1), :] for k in range(routes.shape[0])]
    weights[e] = sum(jnp.where(hit, route_weight[pl.ds(k, 1), :], 0.0) for k, hit in enumerate(hits))

    with scope("own"):
        pltpu.make_async_copy(full.at[e], full.at[e], local.at[0]).wait()
    with scope("barrier"):
        pl.semaphore_wait(barrier, jnp.where(middle, 5, 4))

    def pieces(s):
        return full.at[s, 0, t], full.at[s, 1, t], full.at[s, 1, td], weights.at[s]

    def along(block, k):
        return slot("along") + block * 4 + k

    for k, piece in enumerate(pieces(e)):
        push("small" if k == 3 else "own", piece, piece, along(z, k), ahead * 2 + c, t)
        copy = plan("relay_w" if k == 3 else "relay", piece, piece, along(z, k), behind * 2 + c, t)
        pl.when(middle)(copy.start)
    push("small", weights.at[e], weights.at[e], slot("side_w"), side, t)
    push("side", full.at[e], full.at[e], slot("side"), side, t)

    def step(dz, k, onto, only=None):
        block = back[dz]
        piece = pieces(block * 2 + c)[k]
        arrival = landing(piece, along(block, k))
        if only is not outer:
            passed = plan("relay_w" if k == 3 else "relay", piece, piece, along(block, k), onto * 2 + c, t)
        copies = []
        if k < 2:
            copies.append(plan("plane", piece, piece, slot("x") + dz * 2 - 2 + k, e, tx))
            copies.append(plan("plane", piece, piece, slot("y") + dz * 2 - 2 + k, e, ty))
        if k == 3:
            copies.append(plan("small", piece, piece, slot("side_w") + dz, side, t))
        else:
            copies.append(plan("side", piece, piece, slot("side") + dz, side, t))

        def run():
            arrival.wait_recv()
            if only is None:
                pl.when(middle)(passed.start)
            elif only is middle:
                passed.start()
            for copy in copies:
                copy.start()

        with scope(f"z{k}_{dz}{'' if only is None else 'm' if only is middle else 'o'}"):
            run() if only is None else pl.when(only)(run)

    def near(k):
        step(1, k, ahead)
        step(3, k, behind, middle)

    def far(k):
        step(2, k, behind)

    def last(k):
        step(3, k, behind, outer)

    def aside(dz, a, q):
        piece = full.at[back[dz] * 2 + c, a, q]
        push("side", piece, piece, slot("side") + dz, side, t)

    def relay(dz):
        s = back[dz] * 2 + c
        landed(full.at[s, 0, ty], slot("y") + dz * 2 - 2, f"y0_{dz}")
        piece = full.at[s, 0, ty, :half]
        push("quarters", piece, piece, slot("dx") + dz - 1, e, tx)
        landed(full.at[s, 0, tx], slot("x") + dz * 2 - 2, f"x0_{dz}")
        piece = full.at[s, 0, tx, half:]
        push("quarters", piece, piece, slot("dy") + dz - 1, e, ty)
        aside(dz, 0, ty)
        aside(dz, 0, tx)

    def crossed(dz):
        s = back[dz] * 2 + c
        landed(full.at[s, 1, ty], slot("y") + dz * 2 - 1, f"y1_{dz}")
        aside(dz, 1, ty)
        landed(full.at[s, 1, tx], slot("x") + dz * 2 - 1, f"x1_{dz}")
        aside(dz, 1, tx)

    def diagonal(dz):
        s = back[dz] * 2 + c
        landed(full.at[s, 0, td, :half], slot("dx") + dz - 1, f"dx_{dz}")
        landed(full.at[s, 0, td, half:], slot("dy") + dz - 1, f"dy_{dz}")
        aside(dz, 0, td)

    def nt(a, b):
        return lax.dot_general(a, b, (((1,), (1,)), ((), ())), preferred_element_type=f32)

    def tn(a, b):
        return lax.dot_general(a, b, (((0,), (0,)), ((), ())), preferred_element_type=f32)

    def column(block):
        mine = lax.broadcasted_iota(jnp.int32, (ep, rows), 0) == e
        row = jnp.sum(jnp.where(mine, weights[block], 0.0), axis=0, keepdims=True)
        return jnp.transpose(jnp.broadcast_to(row, (rows, rows)))[:, :1]

    def forward(dz):
        b = back[dz] * 2
        landed(full.at[b + 1 - c], slot("side") + dz, f"side_{dz}")
        landed(weights.at[b + 1 - c], slot("side_w") + dz, f"sidew_{dz}")
        with scope(f"fwd_{dz}"):
            g = u = bk = None
            for q in range(tp):
                span = pl.ds(q * cols, cols)
                xs = jnp.concatenate([full[b, 0, q], full[b + 1, 0, q]], axis=0)
                dy = jnp.concatenate([full[b, 1, q], full[b + 1, 1, q]], axis=0)
                g_q = jnp.dot(xs, gate_v[span, :], preferred_element_type=f32)
                u_q = jnp.dot(xs, up_v[span, :], preferred_element_type=f32)
                b_q = nt(dy, down_v[:, span])
                g, u, bk = (g_q, u_q, b_q) if q == 0 else (g + g_q, u + u_q, bk + b_q)
            w = jnp.concatenate([column(b), column(b + 1)], axis=0)
            sig = jax.nn.sigmoid(g)
            silu = g * sig
            act = silu * u
            d_h = w * bk
            dg = (d_h * u * sig * (1.0 + g * (1.0 - sig))).astype(bf16)
            du = (d_h * silu).astype(bf16)
            aw = (w * act).astype(bf16)
            sums = jnp.sum(act * bk, axis=1, keepdims=True)
            for i in range(2):
                cut = slice(i * rows, (i + 1) * rows)
                d_gate[b + i] = dg[cut]
                d_up[b + i] = du[cut]
                act_w[b + i] = aw[cut]
                score[b + i] = jnp.transpose(jnp.broadcast_to(sums[cut], (rows, rows)))[:8]

    def backward(dz):
        b = back[dz] * 2
        with scope(f"bwd_{dz}"):
            dg = jnp.concatenate([d_gate[b], d_gate[b + 1]], axis=0)
            du = jnp.concatenate([d_up[b], d_up[b + 1]], axis=0)
            for r, q in enumerate((td, tx, ty, t)):
                span = pl.ds(pl.multiple_of(q * cols, cols), cols)
                piece = (nt(dg, gate_v[span, :]) + nt(du, up_v[span, :])).astype(bf16)
                part[b, q] = piece[:rows]
                part[b + 1, q] = piece[rows:]
                push("pair", part.at[b + 1 - c, q], other.at[dz, q], slot("pair") + dz * 3 + max(r - 1, 0), side, t)

    def add(*terms):
        value = terms[0].astype(f32)
        for term in terms[1:]:
            value = value + term.astype(f32)
        return value

    def first(dz):
        s = back[dz] * 2 + c

        def both(q, upper):
            cut = slice(0, half) if upper else slice(half, rows)
            return add(part[s, q, cut], other[dz, q, cut]).astype(bf16)

        landed(other.at[dz, pl.ds(0, 2)], slot("pair") + dz * 3, f"pair0_{dz}")
        top[dz, 3] = both(td, True)
        top[dz, 2] = both(tx, True)
        push("halves", top.at[dz, pl.ds(2, 2)], in_top.at[dz], slot("top") + dz, e, tx)
        landed(other.at[dz, ty], slot("pair") + dz * 3 + 1, f"pair2_{dz}")
        bottom[dz, 3] = both(td, False)
        bottom[dz, 2] = both(ty, False)
        push("halves", bottom.at[dz, pl.ds(2, 2)], in_bottom.at[dz], slot("bottom") + dz, e, ty)
        landed(other.at[dz, t], slot("pair") + dz * 3 + 2, f"pair3_{dz}")
        top[dz, 0] = both(t, True)
        top[dz, 1] = both(ty, True)
        bottom[dz, 0] = both(t, False)
        bottom[dz, 1] = both(tx, False)

    def second(dz):
        landed(in_top.at[dz], slot("top") + dz, f"top_{dz}")
        top[dz, 1] = add(top[dz, 1], in_top[dz, 1]).astype(bf16)
        push("quarters", top.at[dz, 1], last_top.at[dz], slot("last_top") + dz, e, ty)
        landed(in_bottom.at[dz], slot("bottom") + dz, f"bottom_{dz}")
        bottom[dz, 1] = add(bottom[dz, 1], in_bottom[dz, 1]).astype(bf16)
        push("quarters", bottom.at[dz, 1], last_bottom.at[dz], slot("last_bottom") + dz, e, tx)

    def third(dz):
        halves = []
        for cut, mine, got_in, ending, name in (
                (pl.ds(0, half), top, in_top, last_top, "last_top"),
                (pl.ds(half, half), bottom, in_bottom, last_bottom, "last_bottom")):
            landed(ending.at[dz], slot(name) + dz, f"{name}_{dz}")
            value = add(mine[dz, 0], got_in[dz, 0], ending[dz])
            if dz:
                share[dz - 1, cut] = value.astype(bf16)
                push("quarters", share.at[dz - 1, cut], arrived.at[z, cut], slot("share"), back[dz] * 2 + c, t)
            halves.append(value)
        return halves

    def by_width(out, ref, name):
        with scope(name):
            right = ref[...].reshape(ep * rows, ref.shape[2])
            for q in range(tp):
                out[0, pl.ds(q * cols, cols), :] = tn(full[:, 0, q].reshape(ep * rows, cols), right)

    with scope("loads"):
        for copy in loads:
            copy.wait()
    forward(0)
    near(0)
    backward(0)
    near(1)
    first(0)
    relay(1)
    near(2)
    near(3)
    crossed(1)
    far(0)
    diagonal(1)
    second(0)
    forward(1)
    far(1)
    backward(1)
    relay(2)
    first(1)
    far(2)
    far(3)
    crossed(2)
    last(0)
    diagonal(2)
    forward(2)
    last(1)
    backward(2)
    second(1)
    relay(3)
    last(2)
    last(3)
    first(2)
    crossed(3)
    third(1)
    diagonal(3)
    forward(3)
    backward(3)
    second(2)
    score_rows[...] = jnp.concatenate([score[j, :1] for j in range(ep)], axis=0)
    for k in range(1, tp):
        push("small", score_rows, scores.at[t], slot("score"), e, lax.rem(t + k, tp))
    scores[t] = score_rows[...]
    third(2)
    first(3)
    by_width(g_gate, d_gate, "wg_gate")
    landed(scores.at[pl.ds(0, tp - 1)], slot("score"), "score")
    total[...] = add(*[scores[j] for j in range(tp)])
    for k in range(1, ep):
        push("home", total, home.at[e], slot("home"), lax.rem(e + k, ep), t)
    home[e] = total[...]
    by_width(g_up, d_up, "wg_up")
    second(3)
    with scope("wg_down"):
        left = act_w[...].reshape(ep * rows, act_w.shape[2])
        for q in range(tp):
            g_down[0, :, pl.ds(q * cols, cols)] = tn(left, full[:, 1, q].reshape(ep * rows, cols))
    third(3)
    upper, lower = third(0)
    landed(arrived.at[pl.ds(0, nz - 1)], slot("share"), "arrived")
    for k in range(1, nz):
        j = lax.rem(z + k, nz)
        upper = upper + arrived[j, :half].astype(f32)
        lower = lower + arrived[j, half:].astype(f32)
    result[:half] = upper.astype(bf16)
    result[half:] = lower.astype(bf16)
    landed(home.at[pl.ds(0, ep - 1)], slot("home"), "home")
    back_home = jnp.concatenate(
        [jnp.sum(jnp.where(named == e, home[j], 0.0), axis=0, keepdims=True) for j in range(ep)], axis=0)
    for k, hit in enumerate(hits):
        out_home[pl.ds(k, 1), :] = jnp.sum(jnp.where(hit, back_home, 0.0), axis=0, keepdims=True)
    assert sum(n for _, n in names.values()) == got.shape[0]
    with scope("final"):
        drained("pair", other)
        drained("plane", full.at[pl.ds(0, 3), 0])
        drained("side", full.at[pl.ds(0, 4)])
        drained("own", full.at[0, 0, pl.ds(0, 3)])
        drained("halves", full.at[0])
        drained("quarters", full.at[pl.ds(0, 5), 0, pl.ds(0, 2)])
        drained("home", weights.at[pl.ds(0, ep - 1)])
        drained("small", weights)

        @pl.when(middle)
        def _():
            drained("relay", full.at[pl.ds(0, 3), 0])
            drained("relay_w", weights.at[pl.ds(0, 4)])


def deliver(*refs):
    half = (len(refs) - 1) // 2
    copies = [pltpu.make_async_copy(src, dst, refs[-1].at[i])
              for i, (src, dst) in enumerate(zip(refs[:half], refs[half:-1]))]
    for copy in copies:
        copy.start()
    for copy in copies:
        copy.wait()


def dense(tokens, cotangent, routes, route_weight, w_gate, w_up, w_down):
    f32, bf16 = jnp.float32, jnp.bfloat16
    rows, width = tokens.shape
    ep, tp = lax.axis_size("ep"), lax.axis_size("tp")
    cols, half, nz, hidden = width // tp, rows // 2, ep // 2, w_gate.shape[2]
    anywhere, near = pl.BlockSpec(memory_space=pltpu.HBM), pl.BlockSpec(memory_space=pltpu.VMEM)

    def held(space, *arrays):
        return [pltpu.with_memory_space_constraint(x, space) for x in arrays]

    shapes = ((rows, cols), bf16), (routes.T.shape, f32), (w_gate.shape, f32), (w_up.shape, f32), (w_down.shape, f32)
    parts = pl.pallas_call(
        functools.partial(kernel, ep, tp),
        out_shape=tuple(pltpu.VMEM(*shape) for shape in shapes),
        in_specs=[anywhere, anywhere, near, near, anywhere, anywhere, anywhere],
        out_specs=(near,) * 5,
        scratch_shapes=[
            pltpu.VMEM((ep, 2, tp, rows, cols), bf16),
            pltpu.VMEM((width, hidden), bf16),
            pltpu.VMEM((width, hidden), bf16),
            pltpu.VMEM((hidden, width), bf16),
            pltpu.VMEM((ep, ep, rows), f32),
            pltpu.VMEM((ep, tp, rows, cols), bf16),
            pltpu.VMEM((nz, tp, rows, cols), bf16),
            pltpu.VMEM((nz, 4, half, cols), bf16),
            pltpu.VMEM((nz, 4, half, cols), bf16),
            pltpu.VMEM((nz, 2, half, cols), bf16),
            pltpu.VMEM((nz, 2, half, cols), bf16),
            pltpu.VMEM((nz, half, cols), bf16),
            pltpu.VMEM((nz, half, cols), bf16),
            pltpu.VMEM((nz - 1, rows, cols), bf16),
            pltpu.VMEM((nz, rows, cols), bf16),
            pltpu.VMEM((ep, rows, hidden), bf16),
            pltpu.VMEM((ep, rows, hidden), bf16),
            pltpu.VMEM((ep, rows, hidden), bf16),
            pltpu.VMEM((ep, 8, rows), f32),
            pltpu.VMEM((ep, rows), f32),
            pltpu.VMEM((tp, ep, rows), f32),
            pltpu.VMEM((ep, rows), f32),
            pltpu.VMEM((ep, ep, rows), f32),
            pltpu.SemaphoreType.DMA((4,)),
            pltpu.SemaphoreType.DMA((10,)),
            pltpu.SemaphoreType.DMA((19 * nz - 3,)),
        ],
        compiler_params=pltpu.CompilerParams(
            collective_id=0, has_side_effects=True, vmem_limit_bytes=50 * 1024 * 1024),
    )(*held(pltpu.HBM, tokens, cotangent), routes.T, route_weight.T,
      *held(pltpu.HBM, w_gate, w_up, w_down))
    grad_tokens, grw, *grads = pl.pallas_call(
        deliver,
        out_shape=tuple(jax.ShapeDtypeStruct(*shape) for shape in shapes),
        in_specs=[near] * 5,
        out_specs=(anywhere,) * 5,
        scratch_shapes=[pltpu.SemaphoreType.DMA((5,))],
        compiler_params=pltpu.CompilerParams(vmem_limit_bytes=1 << 20),
    )(*held(pltpu.VMEM, *parts))
    return grad_tokens, grw.T, *grads


def on_device(*args):
    rows, width = args[0].shape
    ep, tp = lax.axis_size("ep"), lax.axis_size("tp")
    fits = tp == 4 and ep == 8 and rows % 128 == 0 and 4 * rows * width * ep <= 1 << 24
    return (dense if fits else slotted)(*args)


def solution(mesh):
    return jax.shard_map(
        on_device,
        mesh=mesh,
        in_specs=(
            P("ep", None),
            P("ep", None),
            P("ep", None),
            P("ep", None),
            P("ep", None, "tp"),
            P("ep", None, "tp"),
            P("ep", "tp", None),
        ),
        out_specs=(
            P("ep", "tp"),
            P("ep", None),
            P("ep", None, "tp"),
            P("ep", None, "tp"),
            P("ep", "tp", None),
        ),
        check_vma=False,
    )
```

```python
import functools

import jax
import jax.numpy as jnp
from jax import lax
from jax.experimental import pallas as pl
from jax.experimental.pallas import tpu as pltpu
from jax.sharding import PartitionSpec as P


def slot_index(block_routes, experts, capacity):
    flat_ids = block_routes.reshape(-1)
    onehot = (flat_ids[:, None] == jnp.arange(experts, dtype=jnp.int32)[None, :]).astype(jnp.int32)
    earlier = jnp.cumsum(onehot, axis=0) - onehot
    return flat_ids * capacity + jnp.sum(earlier * onehot, axis=1)


def slotted(tokens, cotangent, routes, route_weight, w_gate, w_up, w_down):
    f32 = jnp.float32
    tok_rows, model_width = tokens.shape
    choices_row = routes.shape[1]
    experts = lax.axis_size("ep")
    capacity = 2 * tok_rows * choices_row // experts
    recv_rows = experts * capacity
    slot_ids = slot_index(routes, experts, capacity)
    send_w = jnp.zeros((recv_rows,), f32).at[slot_ids].set(route_weight.reshape(-1))
    send_x = (
        jnp.zeros((recv_rows, model_width), jnp.bfloat16)
        .at[slot_ids]
        .set(jnp.repeat(tokens, choices_row, axis=0))
    )
    send_dy = (
        jnp.zeros((recv_rows, model_width), jnp.bfloat16)
        .at[slot_ids]
        .set(jnp.repeat(cotangent, choices_row, axis=0))
    )
    got_x = lax.all_to_all(
        send_x.reshape(experts, capacity, model_width),
        "ep",
        split_axis=0,
        concat_axis=0,
        tiled=True,
    )
    got_dy, got_w = (
        lax.all_to_all(
            send_dy.reshape(experts, capacity, model_width),
            "ep",
            split_axis=0,
            concat_axis=0,
            tiled=True,
        ),
        lax.all_to_all(
            send_w.reshape(experts, capacity, 1).astype(jnp.bfloat16),
            "ep",
            split_axis=0,
            concat_axis=0,
            tiled=True,
        ).astype(jnp.float32),
    )
    rows_x = got_x.reshape(recv_rows, model_width)
    rows_dy = got_dy.reshape(recv_rows, model_width)
    rows_w = got_w.reshape(recv_rows)
    gate_w = w_gate[0]
    up_w = w_up[0]
    down_w = w_down[0]
    gate_pre = jnp.dot(rows_x, gate_w, preferred_element_type=f32)
    up_pre = jnp.dot(rows_x, up_w, preferred_element_type=f32)
    gate_sig = jax.nn.sigmoid(gate_pre)
    act_full = gate_pre * gate_sig * up_pre
    act = act_full.astype(jnp.bfloat16)
    back_hidden = jnp.einsum("rd,fd->rf", rows_dy, down_w, preferred_element_type=f32)
    weighted_cot = (rows_w[:, None] * rows_dy.astype(f32)).astype(jnp.bfloat16)
    d_hidden = rows_w[:, None] * back_hidden
    d_gate = (d_hidden * up_pre * gate_sig * (1.0 + gate_pre * (1.0 - gate_sig))).astype(
        jnp.bfloat16
    )
    d_up = (d_hidden * gate_pre * gate_sig).astype(jnp.bfloat16)
    gate_part = jnp.sum(act_full * back_hidden, axis=1)
    token_part = jnp.einsum("rf,df->rd", d_gate, gate_w, preferred_element_type=f32)
    token_part = token_part + jnp.einsum("rf,df->rd", d_up, up_w, preferred_element_type=f32)
    grad_gate = jnp.einsum("rd,rf->df", rows_x, d_gate, preferred_element_type=f32)[None]
    grad_up = jnp.einsum("rd,rf->df", rows_x, d_up, preferred_element_type=f32)[None]
    grad_down = jnp.einsum("rf,rd->fd", act, weighted_cot, preferred_element_type=f32)[None]
    rounded_part = token_part.astype(jnp.bfloat16).astype(f32)
    shares = lax.psum_scatter(
        rounded_part.astype(jnp.bfloat16), "tp", scatter_dimension=1, tiled=True
    )
    gate_total = lax.psum(gate_part, "tp")
    back_x, back_gate = (
        lax.all_to_all(
            shares.reshape(experts, capacity, -1), "ep", split_axis=0, concat_axis=0, tiled=True
        ),
        lax.all_to_all(
            gate_total.reshape(experts, capacity).astype(jnp.bfloat16),
            "ep",
            split_axis=0,
            concat_axis=0,
            tiled=True,
        ).astype(jnp.float32),
    )
    picked = back_x.reshape(recv_rows, -1)[slot_ids].astype(f32).reshape(tok_rows, choices_row, -1)
    grad_route_weight = back_gate.reshape(recv_rows)[slot_ids].reshape(tok_rows, choices_row)
    grad_tokens = jnp.sum(picked, axis=1).astype(jnp.bfloat16)
    return (grad_tokens, grad_route_weight, grad_gate, grad_up, grad_down)


ORDER = (
    ("fwd", 0), ("near", 0), ("near", 1), ("bwd", 0), ("near", 2), ("relayx", 1), ("relayy", 1), ("near", 3),
    ("far", 0), ("far", 1), ("crossed", 1), ("diag", 1), ("far", 2), ("near", 4), ("far", 3), ("last", 0),
    ("fwd", 1), ("last", 1), ("bwd", 1), ("relayx", 2), ("relayy", 2), ("last", 2), ("hand", 1),
    ("relayx", 3), ("crossed", 2), ("relayy", 3), ("far", 4), ("diag", 2), ("last", 3), ("fwd", 2),
    ("bwd", 2), ("diag", 3), ("first", 2), ("crossed", 3), ("last", 4), ("firstB", 2), ("fwd", 3),
    ("second", 2), ("bwd", 3), ("tally",), ("first", 3), ("wg", 2), ("firstB", 3), ("third", 2), ("wg", 1),
    ("homeward",), ("second", 3), ("first", 0), ("firstB", 0), ("third", 3), ("second", 0), ("wg", 3),
    ("third", 0),
)


def kernel(ep, tp, tokens, cotangent, routes, route_weight, w_gate, w_up, w_down,
           result, out_home, g_gate, g_up, g_down,
           full, gate_v, up_v, down_v, weights, part, other, top, bottom,
           in_top, in_bottom, last_top, last_bottom, share, arrived, early,
           d_gate, d_up, act_w, score, score_rows, scores, total, home,
           local, sent, got):
    f32, bf16 = jnp.float32, jnp.bfloat16
    rows, width = tokens.shape
    cols = width // tp
    half = rows // 2
    nz = ep // 2
    e, t = lax.axis_index("ep"), lax.axis_index("tp")
    z, c = e // 2, lax.rem(e, 2)
    y, x = t // 2, lax.rem(t, 2)
    side = z * 2 + 1 - c
    tx, ty = y * 2 + 1 - x, (1 - y) * 2 + x
    td = (1 - y) * 2 + 1 - x
    onward = jnp.where(z < nz // 2, 1, -1)
    middle = jnp.logical_and(z > 0, z < nz - 1)
    outer = jnp.logical_not(middle)
    ahead, behind = z + onward, z - jnp.where(middle, onward, -onward)
    back = [z, ahead, z + 2 * onward, z + jnp.where(middle, -1, 3) * onward]
    groups = {name: i for i, name in enumerate(
        ("pair", "plane", "side", "own", "hand", "quarters", "home", "small", "relay", "relay_w"))}
    names = {}

    def scope(name):
        return jax.named_scope(name)

    def slot(name, count=1):
        if name not in names:
            names[name] = sum(n for _, n in names.values()), count
        return names[name][0]

    def plan(group, src, dst, slot_at, to_e, to_t):
        return pltpu.make_async_remote_copy(
            src_ref=src, dst_ref=dst, send_sem=sent.at[groups[group]], recv_sem=got.at[slot_at],
            device_id={"ep": to_e, "tp": to_t}, device_id_type=pl.DeviceIdType.MESH)

    def push(*args):
        plan(*args).start()

    def drained(group, ref):
        pltpu.make_async_remote_copy(
            src_ref=ref, dst_ref=ref, send_sem=sent.at[groups[group]], recv_sem=got.at[0],
            device_id={"ep": side, "tp": t}, device_id_type=pl.DeviceIdType.MESH).wait_send()

    def landing(dst, slot_at):
        return pltpu.make_async_remote_copy(
            src_ref=dst, dst_ref=dst, send_sem=sent.at[0], recv_sem=got.at[slot_at],
            device_id={"ep": side, "tp": t}, device_id_type=pl.DeviceIdType.MESH)

    def landed(dst, slot_at, label="w"):
        with scope(label):
            landing(dst, slot_at).wait_recv()

    own = [pltpu.make_async_copy(ref.at[:, pl.ds(q * cols, cols)], full.at[e, a, q], local.at[0])
           for a, ref in enumerate((tokens, cotangent)) for q in range(tp)]
    loads = [pltpu.make_async_copy(src.at[0], dst, local.at[1 + i])
             for i, (src, dst) in enumerate(((w_gate, gate_v), (w_up, up_v), (w_down, down_v)))]
    for copy in own + loads:
        copy.start()
    for name, count in (("along", 6 * nz), ("x", 9), ("y", 9), ("dx", 3), ("dy", 3), ("side", 4), ("side_w", 4),
                        ("pair", 4), ("pairs", 4), ("top", 4), ("tops", 4), ("bottom", 4), ("bottoms", 4),
                        ("last_top", 4), ("last_bottom", 4), ("early", 1), ("share", 1), ("score", 1), ("home", 1)):
        slot(name, count)

    barrier = pltpu.get_barrier_semaphore()

    def greet(to_e, to_t):
        pl.semaphore_signal(barrier, inc=1, device_id={"ep": to_e, "tp": to_t},
                            device_id_type=pl.DeviceIdType.MESH)

    greet(side, t)
    greet(e, tx)
    greet(e, ty)
    greet(ahead * 2 + c, t)
    pl.when(middle)(lambda: greet(behind * 2 + c, t))

    named = lax.broadcasted_iota(jnp.int32, (ep, rows), 0)
    hits = [named == routes[pl.ds(k, 1), :] for k in range(routes.shape[0])]
    weights[e] = sum(jnp.where(hit, route_weight[pl.ds(k, 1), :], 0.0) for k, hit in enumerate(hits))

    @pl.when(outer)
    def _():
        early[...] = jnp.zeros_like(early)

    with scope("own"):
        pltpu.make_async_copy(full.at[e], full.at[e], local.at[0]).wait()
    with scope("barrier"):
        pl.semaphore_wait(barrier, jnp.where(middle, 5, 4))

    def pieces(s):
        return (full.at[s, 0, t, :half], full.at[s, 0, t, half:], full.at[s, 1, t, :half], full.at[s, 1, t, half:],
                full.at[s, 1, td], weights.at[s])

    def along(block, k):
        return slot("along") + block * 6 + k

    for k, piece in enumerate(pieces(e)):
        push("small" if k == 5 else "own", piece, piece, along(z, k), ahead * 2 + c, t)
        copy = plan("relay_w" if k == 5 else "relay", piece, piece, along(z, k), behind * 2 + c, t)
        pl.when(middle)(copy.start)
    push("small", weights.at[e], weights.at[e], slot("side_w"), side, t)
    push("side", full.at[e], full.at[e], slot("side"), side, t)

    def step(dz, k, onto, only=None):
        block = back[dz]
        s = block * 2 + c
        piece = pieces(s)[k]
        arrival = landing(piece, along(block, k))
        copies = []
        if only is not outer:
            passed = plan("relay_w" if k == 5 else "relay", piece, piece, along(block, k), onto * 2 + c, t)
        if k < 4:
            to = dz * 3 - 3 + min(k, 2)
            copies.append(plan("plane", piece, piece, slot("x") + to, e, tx))
            copies.append(plan("plane", piece, piece, slot("y") + to, e, ty))
        if k == 5:
            copies.append(plan("small", piece, piece, slot("side_w") + dz, side, t))
        elif k % 2 or k == 4:
            whole = {1: full.at[s, 0, t], 3: full.at[s, 1, t], 4: piece}[k]
            copies.append(plan("side", whole, whole, slot("side") + dz, side, t))

        def run():
            arrival.wait_recv()
            if only is None:
                pl.when(middle)(passed.start)
            elif only is middle:
                passed.start()
            for copy in copies:
                copy.start()

        with scope(f"z{k}_{dz}{'' if only is None else 'm' if only is middle else 'o'}"):
            run() if only is None else pl.when(only)(run)

    def near(k):
        for k in (4, 5) if k == 4 else (k,):
            step(1, k, behind)
            step(3, k, ahead, middle)

    def far(k):
        for k in (4, 5) if k == 4 else (k,):
            step(2, k, behind)

    def last(k):
        for k in (4, 5) if k == 4 else (k,):
            step(3, k, behind, outer)

    def aside(dz, a, q):
        piece = full.at[back[dz] * 2 + c, a, q]
        push("side", piece, piece, slot("side") + dz, side, t)

    def relayx(dz):
        piece = full.at[back[dz] * 2 + c, 0, ty, :half]
        landed(piece, slot("y") + dz * 3 - 3, f"y0_{dz}")
        push("quarters", piece, piece, slot("dx") + dz - 1, e, tx)

    def relayy(dz):
        s = back[dz] * 2 + c
        piece = full.at[s, 0, tx, half:]
        landed(piece, slot("x") + dz * 3 - 2, f"x1_{dz}")
        push("quarters", piece, piece, slot("dy") + dz - 1, e, ty)
        landed(full.at[s, 0, ty, half:], slot("y") + dz * 3 - 2, f"y1_{dz}")
        aside(dz, 0, ty)
        landed(full.at[s, 0, tx, :half], slot("x") + dz * 3 - 3, f"x0_{dz}")
        aside(dz, 0, tx)

    def crossed(dz):
        s = back[dz] * 2 + c
        landed(full.at[s, 1, ty], slot("y") + dz * 3 - 1, f"y2_{dz}")
        aside(dz, 1, ty)
        landed(full.at[s, 1, tx], slot("x") + dz * 3 - 1, f"x2_{dz}")
        aside(dz, 1, tx)

    def diag(dz):
        s = back[dz] * 2 + c
        landed(full.at[s, 0, td, :half], slot("dx") + dz - 1, f"dx_{dz}")
        landed(full.at[s, 0, td, half:], slot("dy") + dz - 1, f"dy_{dz}")
        aside(dz, 0, td)

    def nt(a, b):
        return lax.dot_general(a, b, (((1,), (1,)), ((), ())), preferred_element_type=f32)

    def tn(a, b):
        return lax.dot_general(a, b, (((0,), (0,)), ((), ())), preferred_element_type=f32)

    def column(block):
        mine = lax.broadcasted_iota(jnp.int32, (ep, rows), 0) == e
        row = jnp.sum(jnp.where(mine, weights[block], 0.0), axis=0, keepdims=True)
        return jnp.transpose(jnp.broadcast_to(row, (rows, rows)))[:, :1]

    def fwd(dz):
        b = back[dz] * 2
        landed(full.at[b + 1 - c], slot("side") + dz, f"side_{dz}")
        landed(weights.at[b + 1 - c], slot("side_w") + dz, f"sidew_{dz}")
        with scope(f"fwd_{dz}"):
            g = u = bk = None
            for q in range(tp):
                span = pl.ds(q * cols, cols)
                xs = jnp.concatenate([full[b, 0, q], full[b + 1, 0, q]], axis=0)
                dy = jnp.concatenate([full[b, 1, q], full[b + 1, 1, q]], axis=0)
                g_q = jnp.dot(xs, gate_v[span, :], preferred_element_type=f32)
                u_q = jnp.dot(xs, up_v[span, :], preferred_element_type=f32)
                b_q = nt(dy, down_v[:, span])
                g, u, bk = (g_q, u_q, b_q) if q == 0 else (g + g_q, u + u_q, bk + b_q)
            w = jnp.concatenate([column(b), column(b + 1)], axis=0)
            sig = jax.nn.sigmoid(g)
            silu = g * sig
            act = silu * u
            d_h = w * bk
            dg = (d_h * u * sig * (1.0 + g * (1.0 - sig))).astype(bf16)
            du = (d_h * silu).astype(bf16)
            aw = (w * act).astype(bf16)
            sums = jnp.sum(act * bk, axis=1, keepdims=True)
            for i in range(2):
                cut = slice(i * rows, (i + 1) * rows)
                d_gate[b + i] = dg[cut]
                d_up[b + i] = du[cut]
                act_w[b + i] = aw[cut]
                score[b + i] = jnp.transpose(jnp.broadcast_to(sums[cut], (rows, rows)))[:8]

    def bwd(dz):
        b = back[dz] * 2
        with scope(f"bwd_{dz}"):
            dg = jnp.concatenate([d_gate[b], d_gate[b + 1]], axis=0)
            du = jnp.concatenate([d_up[b], d_up[b + 1]], axis=0)
            for r, q in enumerate((td, tx, ty, t)):
                span = pl.ds(pl.multiple_of(q * cols, cols), cols)
                piece = (nt(dg, gate_v[span, :]) + nt(du, up_v[span, :])).astype(bf16)
                part[b, q] = piece[:rows]
                part[b + 1, q] = piece[rows:]
                push("pair", part.at[b + 1 - c, q], other.at[dz, q], slot("pairs" if r else "pair") + dz, side, t)

    def add(*terms):
        value = terms[0].astype(f32)
        for term in terms[1:]:
            value = value + term.astype(f32)
        return value

    def paired(dz, q, cut=slice(None)):
        terms = [part[back[dz] * 2 + c, q, cut], other[dz, q, cut]]
        return add(*terms, *([early[0, q, cut], early[1, q, cut]] if dz == 0 else [])).astype(bf16)

    upper, lower = slice(0, half), slice(half, rows)

    def hand(dz):
        landed(other.at[dz, td], slot("pair") + dz, f"pair_{dz}")
        landed(other.at[dz, pl.ds(0, 3)], slot("pairs") + dz, f"pairs_{dz}")
        s = back[dz] * 2 + c
        for q in range(tp):
            part[s, q] = paired(dz, q)
            push("hand", part.at[s, q], early.at[jnp.where(middle, 1, 0), q], slot("early"), ahead * 2 + c, t)

    def first(dz):
        landed(other.at[dz, td], slot("pair") + dz, f"pair_{dz}")
        if dz == 0:
            with scope("early"):
                pl.when(middle)(landing(early, slot("early")).wait_recv)
        top[dz, 3] = paired(dz, td, upper)
        push("quarters", top.at[dz, 3], in_top.at[dz, 1], slot("top") + dz, e, tx)
        bottom[dz, 3] = paired(dz, td, lower)
        push("quarters", bottom.at[dz, 3], in_bottom.at[dz, 1], slot("bottom") + dz, e, ty)

    def firstB(dz):
        landed(other.at[dz, pl.ds(0, 3)], slot("pairs") + dz, f"pairs_{dz}")
        top[dz, 2] = paired(dz, tx, upper)
        push("quarters", top.at[dz, 2], in_top.at[dz, 0], slot("tops") + dz, e, tx)
        bottom[dz, 2] = paired(dz, ty, lower)
        push("quarters", bottom.at[dz, 2], in_bottom.at[dz, 0], slot("bottoms") + dz, e, ty)
        top[dz, 1] = paired(dz, ty, upper)
        bottom[dz, 1] = paired(dz, tx, lower)
        top[dz, 0] = paired(dz, t, upper)
        bottom[dz, 0] = paired(dz, t, lower)

    def second(dz):
        landed(in_top.at[dz, 1], slot("top") + dz, f"top_{dz}")
        top[dz, 1] = add(top[dz, 1], in_top[dz, 1]).astype(bf16)
        push("quarters", top.at[dz, 1], last_top.at[dz], slot("last_top") + dz, e, ty)
        landed(in_bottom.at[dz, 1], slot("bottom") + dz, f"bottom_{dz}")
        bottom[dz, 1] = add(bottom[dz, 1], in_bottom[dz, 1]).astype(bf16)
        push("quarters", bottom.at[dz, 1], last_bottom.at[dz], slot("last_bottom") + dz, e, tx)

    kept = []

    def third(dz):
        for cut, mine, got_in, ending, name in (
                (pl.ds(0, half), top, in_top, last_top, "top"), (pl.ds(half, half), bottom, in_bottom, last_bottom, "bottom")):
            landed(got_in.at[dz, 0], slot(name + "s") + dz, f"{name}s_{dz}")
            landed(ending.at[dz], slot("last_" + name) + dz, f"last_{name}_{dz}")
            value = add(mine[dz, 0], got_in[dz, 0], ending[dz])
            if dz:
                share[dz - 2, cut] = value.astype(bf16)
                push("quarters", share.at[dz - 2, cut], arrived.at[z, cut], slot("share"), back[dz] * 2 + c, t)
            else:
                kept.append(value)

    def by_width(out, ref, name):
        with scope(name):
            right = ref[...].reshape(ep * rows, ref.shape[2])
            for q in range(tp):
                out[0, pl.ds(q * cols, cols), :] = tn(full[:, 0, q].reshape(ep * rows, cols), right)

    with scope("loads"):
        for copy in loads:
            copy.wait()
    def wg(i):
        if i == 1:
            by_width(g_gate, d_gate, "wg_gate")
        elif i == 2:
            by_width(g_up, d_up, "wg_up")
        else:
            with scope("wg_down"):
                left = act_w[...].reshape(ep * rows, act_w.shape[2])
                for q in range(tp):
                    g_down[0, :, pl.ds(q * cols, cols)] = tn(left, full[:, 1, q].reshape(ep * rows, cols))

    def tally():
        score_rows[...] = jnp.concatenate([score[j, :1] for j in range(ep)], axis=0)
        for k in range(1, tp):
            push("small", score_rows, scores.at[t], slot("score"), e, lax.rem(t + k, tp))
        scores[t] = score_rows[...]

    def homeward():
        landed(scores.at[pl.ds(0, tp - 1)], slot("score"), "score")
        total[...] = add(*[scores[j] for j in range(tp)])
        for k in range(1, ep):
            push("home", total, home.at[e], slot("home"), lax.rem(e + k, ep), t)
        home[e] = total[...]

    steps = locals()
    for name, *where in ORDER:
        steps[name](*where)

    @pl.when(middle)
    def _():
        landed(arrived.at[pl.ds(0, 1)], slot("share"), "arrived_m")
        for cut, value in zip((upper, lower), kept):
            result[cut] = add(value, arrived[back[2], cut]).astype(bf16)

    @pl.when(outer)
    def _():
        landed(arrived.at[pl.ds(0, nz - 1)], slot("share"), "arrived_o")
        for cut, value in zip((upper, lower), kept):
            result[cut] = add(value, *[arrived[back[i], cut] for i in (1, 2, 3)]).astype(bf16)

    landed(home.at[pl.ds(0, ep - 1)], slot("home"), "home")
    back_home = jnp.concatenate(
        [jnp.sum(jnp.where(named == e, home[j], 0.0), axis=0, keepdims=True) for j in range(ep)], axis=0)
    for k, hit in enumerate(hits):
        out_home[pl.ds(k, 1), :] = jnp.sum(jnp.where(hit, back_home, 0.0), axis=0, keepdims=True)
    assert sum(n for _, n in names.values()) == got.shape[0]
    with scope("final"):
        drained("pair", other)
        drained("plane", full.at[pl.ds(0, 3), 0])
        drained("side", full.at[pl.ds(0, 4)])
        drained("own", full.at[0, 0, pl.ds(0, 3)])
        drained("hand", full.at[0, 0])
        drained("quarters", full.at[pl.ds(0, 7), 0, pl.ds(0, 2)])
        drained("home", weights.at[pl.ds(0, ep - 1)])
        drained("small", weights)

        @pl.when(middle)
        def _():
            drained("relay", full.at[pl.ds(0, 3), 0])
            drained("relay_w", weights.at[pl.ds(0, 4)])


def deliver(*refs):
    half = (len(refs) - 1) // 2
    copies = [pltpu.make_async_copy(src, dst, refs[-1].at[i])
              for i, (src, dst) in enumerate(zip(refs[:half], refs[half:-1]))]
    for copy in copies:
        copy.start()
    for copy in copies:
        copy.wait()


def dense(tokens, cotangent, routes, route_weight, w_gate, w_up, w_down):
    f32, bf16 = jnp.float32, jnp.bfloat16
    rows, width = tokens.shape
    ep, tp = lax.axis_size("ep"), lax.axis_size("tp")
    cols, half, nz, hidden = width // tp, rows // 2, ep // 2, w_gate.shape[2]
    anywhere, near = pl.BlockSpec(memory_space=pltpu.HBM), pl.BlockSpec(memory_space=pltpu.VMEM)

    def held(space, *arrays):
        return [pltpu.with_memory_space_constraint(x, space) for x in arrays]

    shapes = ((rows, cols), bf16), (routes.T.shape, f32), (w_gate.shape, f32), (w_up.shape, f32), (w_down.shape, f32)
    parts = pl.pallas_call(
        functools.partial(kernel, ep, tp),
        out_shape=tuple(pltpu.VMEM(*shape) for shape in shapes),
        in_specs=[anywhere, anywhere, near, near, anywhere, anywhere, anywhere],
        out_specs=(near,) * 5,
        scratch_shapes=[
            pltpu.VMEM((ep, 2, tp, rows, cols), bf16),
            pltpu.VMEM((width, hidden), bf16),
            pltpu.VMEM((width, hidden), bf16),
            pltpu.VMEM((hidden, width), bf16),
            pltpu.VMEM((ep, ep, rows), f32),
            pltpu.VMEM((ep, tp, rows, cols), bf16),
            pltpu.VMEM((nz, tp, rows, cols), bf16),
            pltpu.VMEM((nz, 4, half, cols), bf16),
            pltpu.VMEM((nz, 4, half, cols), bf16),
            pltpu.VMEM((nz, 2, half, cols), bf16),
            pltpu.VMEM((nz, 2, half, cols), bf16),
            pltpu.VMEM((nz, half, cols), bf16),
            pltpu.VMEM((nz, half, cols), bf16),
            pltpu.VMEM((2, rows, cols), bf16),
            pltpu.VMEM((nz, rows, cols), bf16),
            pltpu.VMEM((2, tp, rows, cols), bf16),
            pltpu.VMEM((ep, rows, hidden), bf16),
            pltpu.VMEM((ep, rows, hidden), bf16),
            pltpu.VMEM((ep, rows, hidden), bf16),
            pltpu.VMEM((ep, 8, rows), f32),
            pltpu.VMEM((ep, rows), f32),
            pltpu.VMEM((tp, ep, rows), f32),
            pltpu.VMEM((ep, rows), f32),
            pltpu.VMEM((ep, ep, rows), f32),
            pltpu.SemaphoreType.DMA((4,)),
            pltpu.SemaphoreType.DMA((10,)),
            pltpu.SemaphoreType.DMA((92,)),
        ],
        compiler_params=pltpu.CompilerParams(
            collective_id=0, has_side_effects=True, vmem_limit_bytes=50 * 1024 * 1024),
    )(*held(pltpu.HBM, tokens, cotangent), routes.T, route_weight.T,
      *held(pltpu.HBM, w_gate, w_up, w_down))
    grad_tokens, grw, *grads = pl.pallas_call(
        deliver,
        out_shape=tuple(jax.ShapeDtypeStruct(*shape) for shape in shapes),
        in_specs=[near] * 5,
        out_specs=(anywhere,) * 5,
        scratch_shapes=[pltpu.SemaphoreType.DMA((5,))],
        compiler_params=pltpu.CompilerParams(vmem_limit_bytes=1 << 20),
    )(*held(pltpu.VMEM, *parts))
    return grad_tokens, grw.T, *grads


def on_device(*args):
    rows, width = args[0].shape
    ep, tp = lax.axis_size("ep"), lax.axis_size("tp")
    fits = tp == 4 and ep == 8 and rows % 128 == 0 and 4 * rows * width * ep <= 1 << 24
    return (dense if fits else slotted)(*args)


def solution(mesh):
    return jax.shard_map(
        on_device,
        mesh=mesh,
        in_specs=(
            P("ep", None),
            P("ep", None),
            P("ep", None),
            P("ep", None),
            P("ep", None, "tp"),
            P("ep", None, "tp"),
            P("ep", "tp", None),
        ),
        out_specs=(
            P("ep", "tp"),
            P("ep", None),
            P("ep", None, "tp"),
            P("ep", None, "tp"),
            P("ep", "tp", None),
        ),
        check_vma=False,
    )
```

```python
import functools

import jax
import jax.numpy as jnp
from jax import lax
from jax.experimental import pallas as pl
from jax.experimental.pallas import tpu as pltpu
from jax.sharding import PartitionSpec as P


def slot_index(block_routes, experts, capacity):
    flat_ids = block_routes.reshape(-1)
    onehot = (flat_ids[:, None] == jnp.arange(experts, dtype=jnp.int32)[None, :]).astype(jnp.int32)
    earlier = jnp.cumsum(onehot, axis=0) - onehot
    return flat_ids * capacity + jnp.sum(earlier * onehot, axis=1)


def slotted(tokens, cotangent, routes, route_weight, w_gate, w_up, w_down):
    f32 = jnp.float32
    tok_rows, model_width = tokens.shape
    choices_row = routes.shape[1]
    experts = lax.axis_size("ep")
    capacity = 2 * tok_rows * choices_row // experts
    recv_rows = experts * capacity
    slot_ids = slot_index(routes, experts, capacity)
    send_w = jnp.zeros((recv_rows,), f32).at[slot_ids].set(route_weight.reshape(-1))
    send_x = (
        jnp.zeros((recv_rows, model_width), jnp.bfloat16)
        .at[slot_ids]
        .set(jnp.repeat(tokens, choices_row, axis=0))
    )
    send_dy = (
        jnp.zeros((recv_rows, model_width), jnp.bfloat16)
        .at[slot_ids]
        .set(jnp.repeat(cotangent, choices_row, axis=0))
    )
    got_x = lax.all_to_all(
        send_x.reshape(experts, capacity, model_width),
        "ep",
        split_axis=0,
        concat_axis=0,
        tiled=True,
    )
    got_dy, got_w = (
        lax.all_to_all(
            send_dy.reshape(experts, capacity, model_width),
            "ep",
            split_axis=0,
            concat_axis=0,
            tiled=True,
        ),
        lax.all_to_all(
            send_w.reshape(experts, capacity, 1).astype(jnp.bfloat16),
            "ep",
            split_axis=0,
            concat_axis=0,
            tiled=True,
        ).astype(jnp.float32),
    )
    rows_x = got_x.reshape(recv_rows, model_width)
    rows_dy = got_dy.reshape(recv_rows, model_width)
    rows_w = got_w.reshape(recv_rows)
    gate_w = w_gate[0]
    up_w = w_up[0]
    down_w = w_down[0]
    gate_pre = jnp.dot(rows_x, gate_w, preferred_element_type=f32)
    up_pre = jnp.dot(rows_x, up_w, preferred_element_type=f32)
    gate_sig = jax.nn.sigmoid(gate_pre)
    act_full = gate_pre * gate_sig * up_pre
    act = act_full.astype(jnp.bfloat16)
    back_hidden = jnp.einsum("rd,fd->rf", rows_dy, down_w, preferred_element_type=f32)
    weighted_cot = (rows_w[:, None] * rows_dy.astype(f32)).astype(jnp.bfloat16)
    d_hidden = rows_w[:, None] * back_hidden
    d_gate = (d_hidden * up_pre * gate_sig * (1.0 + gate_pre * (1.0 - gate_sig))).astype(
        jnp.bfloat16
    )
    d_up = (d_hidden * gate_pre * gate_sig).astype(jnp.bfloat16)
    gate_part = jnp.sum(act_full * back_hidden, axis=1)
    token_part = jnp.einsum("rf,df->rd", d_gate, gate_w, preferred_element_type=f32)
    token_part = token_part + jnp.einsum("rf,df->rd", d_up, up_w, preferred_element_type=f32)
    grad_gate = jnp.einsum("rd,rf->df", rows_x, d_gate, preferred_element_type=f32)[None]
    grad_up = jnp.einsum("rd,rf->df", rows_x, d_up, preferred_element_type=f32)[None]
    grad_down = jnp.einsum("rf,rd->fd", act, weighted_cot, preferred_element_type=f32)[None]
    rounded_part = token_part.astype(jnp.bfloat16).astype(f32)
    shares = lax.psum_scatter(
        rounded_part.astype(jnp.bfloat16), "tp", scatter_dimension=1, tiled=True
    )
    gate_total = lax.psum(gate_part, "tp")
    back_x, back_gate = (
        lax.all_to_all(
            shares.reshape(experts, capacity, -1), "ep", split_axis=0, concat_axis=0, tiled=True
        ),
        lax.all_to_all(
            gate_total.reshape(experts, capacity).astype(jnp.bfloat16),
            "ep",
            split_axis=0,
            concat_axis=0,
            tiled=True,
        ).astype(jnp.float32),
    )
    picked = back_x.reshape(recv_rows, -1)[slot_ids].astype(f32).reshape(tok_rows, choices_row, -1)
    grad_route_weight = back_gate.reshape(recv_rows)[slot_ids].reshape(tok_rows, choices_row)
    grad_tokens = jnp.sum(picked, axis=1).astype(jnp.bfloat16)
    return (grad_tokens, grad_route_weight, grad_gate, grad_up, grad_down)


def kernel(ep, tp, tokens, cotangent, routes, route_weight, w_gate, w_up, w_down,
           result, out_home, g_gate, g_up, g_down,
           full, in_v, down_v, weights, part, other, top, bottom,
           in_top, in_bottom, last_top, last_bottom, share, arrived, early,
           d_in, act_w, score, score_rows, scores, total, home,
           local, sent, got):
    f32, bf16 = jnp.float32, jnp.bfloat16
    rows, width = tokens.shape
    cols = width // tp
    half = rows // 2
    nz = ep // 2
    e, t = lax.axis_index("ep"), lax.axis_index("tp")
    z, c = e // 2, lax.rem(e, 2)
    y, x = t // 2, lax.rem(t, 2)
    side = z * 2 + 1 - c
    tx, ty = y * 2 + 1 - x, (1 - y) * 2 + x
    td = (1 - y) * 2 + 1 - x
    onward = jnp.where(z < nz // 2, 1, -1)
    middle = jnp.logical_and(z > 0, z < nz - 1)
    outer = jnp.logical_not(middle)
    ahead, behind = z + onward, z - jnp.where(middle, onward, -onward)
    back = [z, ahead, z + 2 * onward, z + jnp.where(middle, -1, 3) * onward]
    groups = {name: i for i, name in enumerate(
        ("pair", "plane", "side", "own", "hand", "quarters", "home", "small", "relay", "relay_w"))}
    names = {}

    def slot(name, count=1):
        if name not in names:
            names[name] = sum(n for _, n in names.values()), count
        return names[name][0]

    def plan(group, src, dst, slot_at, to_e, to_t):
        return pltpu.make_async_remote_copy(
            src_ref=src, dst_ref=dst, send_sem=sent.at[groups[group]], recv_sem=got.at[slot_at],
            device_id={"ep": to_e, "tp": to_t}, device_id_type=pl.DeviceIdType.MESH)

    def push(*args):
        plan(*args).start()

    def drained(group, ref):
        pltpu.make_async_remote_copy(
            src_ref=ref, dst_ref=ref, send_sem=sent.at[groups[group]], recv_sem=got.at[0],
            device_id={"ep": side, "tp": t}, device_id_type=pl.DeviceIdType.MESH).wait_send()

    def landing(dst, slot_at):
        return pltpu.make_async_remote_copy(
            src_ref=dst, dst_ref=dst, send_sem=sent.at[0], recv_sem=got.at[slot_at],
            device_id={"ep": side, "tp": t}, device_id_type=pl.DeviceIdType.MESH)

    def landed(dst, slot_at):
        landing(dst, slot_at).wait_recv()

    barrier = pltpu.get_barrier_semaphore()

    def greet(to_e, to_t):
        pl.semaphore_signal(barrier, inc=1, device_id={"ep": to_e, "tp": to_t},
                            device_id_type=pl.DeviceIdType.MESH)

    own_tiles = [pltpu.make_async_copy(ref.at[:, pl.ds(q * cols, cols)], full.at[e, a, q], local.at[0])
                 for a, ref in enumerate((tokens, cotangent)) for q in range(tp)]
    for copy in own_tiles:
        copy.start()
    greet(ahead * 2 + c, t)
    pl.when(middle)(lambda: greet(behind * 2 + c, t))
    greet(e, tx)
    greet(e, ty)
    greet(side, t)

    for name, count in (("along", 6 * nz), ("x", 9), ("y", 9), ("dx", 3), ("dy", 3), ("side", 4), ("side_w", 4),
                        ("pair", 4), ("pairs", 4), ("top", 3), ("tops", 3), ("bottom", 3), ("bottoms", 3),
                        ("last_top", 3), ("last_bottom", 3), ("early", 1), ("share", 1), ("score", 1), ("home", 1)):
        slot(name, count)

    def summed(name, dz):
        return slot(name) + max(dz - 1, 0)

    named = lax.broadcasted_iota(jnp.int32, (ep, rows), 0)
    hits = [named == routes[pl.ds(k, 1), :] for k in range(routes.shape[0])]
    weights[e] = sum(jnp.where(hit, route_weight[pl.ds(k, 1), :], 0.0) for k, hit in enumerate(hits))
    pltpu.make_async_copy(full.at[e], full.at[e], local.at[0]).wait()
    pl.semaphore_wait(barrier, jnp.where(middle, 5, 4))

    def pieces(s):
        return (full.at[s, 0, t, :half], full.at[s, 0, t, half:], full.at[s, 1, t, :half], full.at[s, 1, t, half:],
                full.at[s, 1, td], weights.at[s])

    def along(block, k):
        return slot("along") + block * 6 + k

    for k, piece in enumerate(pieces(e)):
        push("small" if k == 5 else "own", piece, piece, along(z, k), ahead * 2 + c, t)
        copy = plan("relay_w" if k == 5 else "relay", piece, piece, along(z, k), behind * 2 + c, t)
        pl.when(middle)(copy.start)
    hidden = down_v.shape[0]
    loads = [pltpu.make_async_copy(src.at[0], dst, local.at[1 + i]) for i, (src, dst) in enumerate((
        (w_gate, in_v.at[:, pl.ds(0, hidden)]), (w_up, in_v.at[:, pl.ds(hidden, hidden)]), (w_down, down_v)))]
    for copy in loads:
        copy.start()

    @pl.when(outer)
    def _():
        early[...] = jnp.zeros_like(early)

    def own():
        push("small", weights.at[e], weights.at[e], slot("side_w"), side, t)
        push("side", full.at[e], full.at[e], slot("side"), side, t)
        for copy in loads:
            copy.wait()

    onto = {}

    def step(dz, k):
        if k == 6:
            return
        block = back[dz]
        s = block * 2 + c
        piece = pieces(s)[k]
        landed(piece, along(block, k))
        if dz in onto:
            push("relay_w" if k == 5 else "relay", piece, piece, along(block, k), onto[dz] * 2 + c, t)
        if k < 4:
            to = dz * 3 - 3 + min(k, 2)
            push("plane", piece, piece, slot("x") + to, e, tx)
            push("plane", piece, piece, slot("y") + to, e, ty)
        if k == 5:
            push("small", piece, piece, slot("side_w") + dz, side, t)
        elif k % 2 or k == 4:
            whole = {1: full.at[s, 0, t], 3: full.at[s, 1, t], 4: piece}[k]
            push("side", whole, whole, slot("side") + dz, side, t)
        if k == 4:
            step(dz, 5)

    def near(k):
        step(1, k)

    def far(k):
        step(2, k)

    def last(k):
        step(3, k)

    def aside(dz, a, q):
        piece = full.at[back[dz] * 2 + c, a, q]
        push("side", piece, piece, slot("side") + dz, side, t)

    def relayx(dz):
        piece = full.at[back[dz] * 2 + c, 0, ty, :half]
        landed(piece, slot("y") + dz * 3 - 3)
        push("quarters", piece, piece, slot("dx") + dz - 1, e, tx)

    def relayy(dz):
        s = back[dz] * 2 + c
        piece = full.at[s, 0, tx, half:]
        landed(piece, slot("x") + dz * 3 - 2)
        push("quarters", piece, piece, slot("dy") + dz - 1, e, ty)
        landed(full.at[s, 0, ty, half:], slot("y") + dz * 3 - 2)
        aside(dz, 0, ty)
        landed(full.at[s, 0, tx, :half], slot("x") + dz * 3 - 3)
        aside(dz, 0, tx)

    def crossed(dz):
        s = back[dz] * 2 + c
        landed(full.at[s, 1, ty], slot("y") + dz * 3 - 1)
        aside(dz, 1, ty)
        landed(full.at[s, 1, tx], slot("x") + dz * 3 - 1)
        aside(dz, 1, tx)

    def diag(dz):
        s = back[dz] * 2 + c
        landed(full.at[s, 0, td, :half], slot("dx") + dz - 1)
        landed(full.at[s, 0, td, half:], slot("dy") + dz - 1)
        aside(dz, 0, td)

    def nt(a, b):
        return lax.dot_general(a, b, (((1,), (1,)), ((), ())), preferred_element_type=f32)

    def tn(a, b):
        return lax.dot_general(a, b, (((0,), (0,)), ((), ())), preferred_element_type=f32)

    def column(block):
        mine = lax.broadcasted_iota(jnp.int32, (ep, rows), 0) == e
        row = jnp.sum(jnp.where(mine, weights[block], 0.0), axis=0, keepdims=True)
        return jnp.transpose(jnp.broadcast_to(row, (rows, rows)))[:, :1]

    def fwd(dz):
        b = back[dz] * 2
        landed(full.at[b + 1 - c], slot("side") + dz)
        landed(weights.at[b + 1 - c], slot("side_w") + dz)
        gu = bk = None
        for q in range(tp):
            span = pl.ds(q * cols, cols)
            xs = jnp.concatenate([full[b, 0, q], full[b + 1, 0, q]], axis=0)
            dy = jnp.concatenate([full[b, 1, q], full[b + 1, 1, q]], axis=0)
            gu_q = jnp.dot(xs, in_v[span, :], preferred_element_type=f32)
            b_q = nt(dy, down_v[:, span])
            gu, bk = (gu_q, b_q) if q == 0 else (gu + gu_q, bk + b_q)
        g, u = gu[:, :hidden], gu[:, hidden:]
        w = jnp.concatenate([column(b), column(b + 1)], axis=0)
        sig = jax.nn.sigmoid(g)
        silu = g * sig
        act = silu * u
        d_h = w * bk
        dg = (d_h * u * sig * (1.0 + g * (1.0 - sig))).astype(bf16)
        du = (d_h * silu).astype(bf16)
        aw = (w * act).astype(bf16)
        sums = jnp.sum(act * bk, axis=1, keepdims=True)
        for i in range(2):
            cut = slice(i * rows, (i + 1) * rows)
            d_in[b + i, :, :hidden] = dg[cut]
            d_in[b + i, :, hidden:] = du[cut]
            act_w[b + i] = aw[cut]
            score[b + i] = jnp.transpose(jnp.broadcast_to(sums[cut], (rows, rows)))[:8]

    def bwd(dz):
        b = back[dz] * 2
        d = jnp.concatenate([d_in[b], d_in[b + 1]], axis=0)
        for group, name in (((td,), "pair"), ((tx, ty, t), "pairs")):
            for q in group:
                piece = nt(d, in_v[pl.ds(pl.multiple_of(q * cols, cols), cols), :]).astype(bf16)
                part[b, q] = piece[:rows]
                part[b + 1, q] = piece[rows:]
            for q in group:
                push("pair", part.at[b + 1 - c, q], other.at[dz, q], slot(name) + dz, side, t)

    def add(*terms):
        value = terms[0].astype(f32)
        for term in terms[1:]:
            value = value + term.astype(f32)
        return value

    def paired(dz, q, cut=slice(None)):
        terms = [part[back[dz] * 2 + c, q, cut], other[dz, q, cut]]
        return add(*terms, *([early[0, q, cut], early[1, q, cut]] if dz == 0 else [])).astype(bf16)

    upper, lower = slice(0, half), slice(half, rows)

    def hand(dz):
        landed(other.at[dz, td], slot("pair") + dz)
        landed(other.at[dz, pl.ds(0, 3)], slot("pairs") + dz)
        s = back[dz] * 2 + c
        for q in range(tp):
            part[s, q] = paired(dz, q)
            push("hand", part.at[s, q], early.at[jnp.where(middle, 1, 0), q], slot("early"), ahead * 2 + c, t)

    def first(dz):
        landed(other.at[dz, td], slot("pair") + dz)
        if dz == 0:
            if onto:
                landed(early, slot("early"))
        top[dz, 3] = paired(dz, td, upper)
        push("quarters", top.at[dz, 3], in_top.at[dz, 1], summed("top", dz), e, tx)
        bottom[dz, 3] = paired(dz, td, lower)
        push("quarters", bottom.at[dz, 3], in_bottom.at[dz, 1], summed("bottom", dz), e, ty)

    def firstB(dz):
        landed(other.at[dz, pl.ds(0, 3)], slot("pairs") + dz)
        top[dz, 2] = paired(dz, tx, upper)
        push("quarters", top.at[dz, 2], in_top.at[dz, 0], summed("tops", dz), e, tx)
        bottom[dz, 2] = paired(dz, ty, lower)
        push("quarters", bottom.at[dz, 2], in_bottom.at[dz, 0], summed("bottoms", dz), e, ty)
        top[dz, 1] = paired(dz, ty, upper)
        bottom[dz, 1] = paired(dz, tx, lower)
        top[dz, 0] = paired(dz, t, upper)
        bottom[dz, 0] = paired(dz, t, lower)

    def second(dz):
        landed(in_top.at[dz, 1], summed("top", dz))
        top[dz, 1] = add(top[dz, 1], in_top[dz, 1]).astype(bf16)
        push("quarters", top.at[dz, 1], last_top.at[dz], summed("last_top", dz), e, ty)
        landed(in_bottom.at[dz, 1], summed("bottom", dz))
        bottom[dz, 1] = add(bottom[dz, 1], in_bottom[dz, 1]).astype(bf16)
        push("quarters", bottom.at[dz, 1], last_bottom.at[dz], summed("last_bottom", dz), e, tx)

    kept = []

    def third(dz):
        for cut, mine, got_in, ending, name in (
                (pl.ds(0, half), top, in_top, last_top, "top"), (pl.ds(half, half), bottom, in_bottom, last_bottom, "bottom")):
            landed(got_in.at[dz, 0], summed(name + "s", dz))
            landed(ending.at[dz], summed("last_" + name, dz))
            value = add(mine[dz, 0], got_in[dz, 0], ending[dz])
            if dz:
                share[dz - 2, cut] = value.astype(bf16)
                push("quarters", share.at[dz - 2, cut], arrived.at[z, cut], slot("share"), back[dz] * 2 + c, t)
            else:
                kept.append(value)

    def wg(i):
        if i < 3:
            right = d_in[...].reshape(ep * rows, 2 * hidden)
            for q in range(i * 2 - 2, i * 2):
                both = tn(full[:, 0, q].reshape(ep * rows, cols), right)
                g_gate[0, pl.ds(q * cols, cols), :] = both[:, :hidden]
                g_up[0, pl.ds(q * cols, cols), :] = both[:, hidden:]
        else:
            left = act_w[...].reshape(ep * rows, hidden)
            for q in range(tp):
                g_down[0, :, pl.ds(q * cols, cols)] = tn(left, full[:, 1, q].reshape(ep * rows, cols))

    def tally():
        score_rows[...] = jnp.concatenate([score[j, :1] for j in range(ep)], axis=0)
        for k in range(1, tp):
            push("small", score_rows, scores.at[t], slot("score"), e, lax.rem(t + k, tp))
        scores[t] = score_rows[...]

    def homeward():
        landed(scores.at[pl.ds(0, tp - 1)], slot("score"))
        total[...] = add(*[scores[j] for j in range(tp)])
        for k in range(1, ep):
            push("home", total, home.at[e], slot("home"), lax.rem(e + k, ep), t)
        home[e] = total[...]

    def finish(count, blocks):
        landed(arrived.at[pl.ds(0, count)], slot("share"))
        for cut, value in zip((upper, lower), kept):
            result[cut] = add(value, *[arrived[back[i], cut] for i in blocks]).astype(bf16)
        kept.clear()

    @pl.when(outer)
    def _():
        for act, *where in (
            (own,), (fwd, 0), (near, 0), (near, 1), (near, 2), (near, 3), (relayx, 1), (near, 4), (relayy, 1),
            (far, 0), (far, 1), (diag, 1), (far, 2), (crossed, 1), (relayx, 2), (far, 3), (last, 0), (fwd, 1),
            (relayy, 2), (last, 1), (bwd, 1), (hand, 1), (crossed, 2), (diag, 2), (last, 2), (far, 4), (relayx, 3),
            (relayy, 3), (fwd, 2), (last, 3), (bwd, 2), (diag, 3), (first, 2), (bwd, 0), (last, 4), (crossed, 3),
            (firstB, 2), (second, 2), (fwd, 3), (bwd, 3), (tally,), (first, 3), (third, 2), (wg, 1), (firstB, 3),
            (second, 3), (first, 0), (firstB, 0), (wg, 2), (homeward,), (wg, 3), (third, 3), (second, 0), (third, 0),
        ):
            with jax.named_scope(act.__name__):
                act(*where)
        finish(nz - 1, (1, 2, 3))

    @pl.when(middle)
    def _():
        onto.update({1: behind, 2: behind, 3: ahead})
        for act, *where in (
            (own,), (last, 0), (near, 0), (near, 1), (near, 2), (last, 1), (relayx, 1), (near, 3), (relayy, 1),
            (far, 0), (last, 2), (relayx, 3), (last, 3), (relayy, 3), (far, 1), (fwd, 0), (crossed, 1), (diag, 1),
            (far, 2), (near, 4), (fwd, 1), (last, 4), (far, 3), (bwd, 0), (relayx, 2), (bwd, 1), (crossed, 3),
            (diag, 3), (hand, 1), (relayy, 2), (far, 4), (fwd, 3), (bwd, 3), (first, 3), (crossed, 2), (diag, 2),
            (firstB, 3), (fwd, 2), (second, 3), (bwd, 2), (tally,), (first, 2), (wg, 3), (firstB, 2), (third, 3),
            (wg, 1), (second, 2), (homeward,), (wg, 2), (first, 0), (firstB, 0), (third, 2), (second, 0), (third, 0),
        ):
            with jax.named_scope(act.__name__):
                act(*where)
        finish(1, (2,))

    landed(home.at[pl.ds(0, ep - 1)], slot("home"))
    back_home = jnp.concatenate(
        [jnp.sum(jnp.where(named == e, home[j], 0.0), axis=0, keepdims=True) for j in range(ep)], axis=0)
    for k, hit in enumerate(hits):
        out_home[pl.ds(k, 1), :] = jnp.sum(jnp.where(hit, back_home, 0.0), axis=0, keepdims=True)
    assert sum(n for _, n in names.values()) == got.shape[0]
    drained("pair", other)
    drained("plane", full.at[pl.ds(0, 3), 0])
    drained("side", full.at[pl.ds(0, 4)])
    drained("own", full.at[0, 0, pl.ds(0, 3)])
    drained("hand", full.at[0, 0])
    drained("quarters", full.at[pl.ds(0, 7), 0, pl.ds(0, 2)])
    drained("home", weights.at[pl.ds(0, ep - 1)])
    drained("small", weights)

    @pl.when(middle)
    def _():
        drained("relay", full.at[pl.ds(0, 3), 0])
        drained("relay_w", weights.at[pl.ds(0, 4)])


def deliver(*refs):
    half = (len(refs) - 1) // 2
    copies = [pltpu.make_async_copy(src, dst, refs[-1].at[i])
              for i, (src, dst) in enumerate(zip(refs[:half], refs[half:-1]))]
    for copy in copies:
        copy.start()
    for copy in copies:
        copy.wait()


def dense(tokens, cotangent, routes, route_weight, w_gate, w_up, w_down):
    f32, bf16 = jnp.float32, jnp.bfloat16
    rows, width = tokens.shape
    ep, tp = lax.axis_size("ep"), lax.axis_size("tp")
    cols, half, nz, hidden = width // tp, rows // 2, ep // 2, w_gate.shape[2]
    anywhere, near = pl.BlockSpec(memory_space=pltpu.HBM), pl.BlockSpec(memory_space=pltpu.VMEM)

    def held(space, *arrays):
        return [pltpu.with_memory_space_constraint(x, space) for x in arrays]

    shapes = ((rows, cols), bf16), (routes.T.shape, f32), (w_gate.shape, f32), (w_up.shape, f32), (w_down.shape, f32)
    parts = pl.pallas_call(
        functools.partial(kernel, ep, tp),
        out_shape=tuple(pltpu.VMEM(*shape) for shape in shapes),
        in_specs=[anywhere, anywhere, near, near, anywhere, anywhere, anywhere],
        out_specs=(near,) * 5,
        scratch_shapes=[
            pltpu.VMEM((ep, 2, tp, rows, cols), bf16),
            pltpu.VMEM((width, 2 * hidden), bf16),
            pltpu.VMEM((hidden, width), bf16),
            pltpu.VMEM((ep, ep, rows), f32),
            pltpu.VMEM((ep, tp, rows, cols), bf16),
            pltpu.VMEM((nz, tp, rows, cols), bf16),
            pltpu.VMEM((nz, 4, half, cols), bf16),
            pltpu.VMEM((nz, 4, half, cols), bf16),
            pltpu.VMEM((nz, 2, half, cols), bf16),
            pltpu.VMEM((nz, 2, half, cols), bf16),
            pltpu.VMEM((nz, half, cols), bf16),
            pltpu.VMEM((nz, half, cols), bf16),
            pltpu.VMEM((2, rows, cols), bf16),
            pltpu.VMEM((nz, rows, cols), bf16),
            pltpu.VMEM((2, tp, rows, cols), bf16),
            pltpu.VMEM((ep, rows, 2 * hidden), bf16),
            pltpu.VMEM((ep, rows, hidden), bf16),
            pltpu.VMEM((ep, 8, rows), f32),
            pltpu.VMEM((ep, rows), f32),
            pltpu.VMEM((tp, ep, rows), f32),
            pltpu.VMEM((ep, rows), f32),
            pltpu.VMEM((ep, ep, rows), f32),
            pltpu.SemaphoreType.DMA((4,)),
            pltpu.SemaphoreType.DMA((10,)),
            pltpu.SemaphoreType.DMA((86,)),
        ],
        compiler_params=pltpu.CompilerParams(
            collective_id=0, has_side_effects=True, vmem_limit_bytes=50 * 1024 * 1024),
    )(*held(pltpu.HBM, tokens, cotangent), routes.T, route_weight.T,
      *held(pltpu.HBM, w_gate, w_up, w_down))
    grad_tokens, grw, *grads = pl.pallas_call(
        deliver,
        out_shape=tuple(jax.ShapeDtypeStruct(*shape) for shape in shapes),
        in_specs=[near] * 5,
        out_specs=(anywhere,) * 5,
        scratch_shapes=[pltpu.SemaphoreType.DMA((5,))],
        compiler_params=pltpu.CompilerParams(vmem_limit_bytes=1 << 20),
    )(*held(pltpu.VMEM, *parts))
    return grad_tokens, grw.T, *grads


def on_device(*args):
    rows, width = args[0].shape
    ep, tp = lax.axis_size("ep"), lax.axis_size("tp")
    fits = tp == 4 and ep == 8 and rows % 128 == 0 and 4 * rows * width * ep <= 1 << 24
    return (dense if fits else slotted)(*args)


def solution(mesh):
    return jax.shard_map(
        on_device,
        mesh=mesh,
        in_specs=(
            P("ep", None),
            P("ep", None),
            P("ep", None),
            P("ep", None),
            P("ep", None, "tp"),
            P("ep", None, "tp"),
            P("ep", "tp", None),
        ),
        out_specs=(
            P("ep", "tp"),
            P("ep", None),
            P("ep", None, "tp"),
            P("ep", None, "tp"),
            P("ep", "tp", None),
        ),
        check_vma=False,
    )
```

```python
import functools

import jax
import jax.numpy as jnp
from jax import lax
from jax.experimental import pallas as pl
from jax.experimental.pallas import tpu as pltpu
from jax.sharding import PartitionSpec as P


def slot_index(block_routes, experts, capacity):
    flat_ids = block_routes.reshape(-1)
    onehot = (flat_ids[:, None] == jnp.arange(experts, dtype=jnp.int32)[None, :]).astype(jnp.int32)
    earlier = jnp.cumsum(onehot, axis=0) - onehot
    return flat_ids * capacity + jnp.sum(earlier * onehot, axis=1)


def slotted(tokens, cotangent, routes, route_weight, w_gate, w_up, w_down):
    f32 = jnp.float32
    tok_rows, model_width = tokens.shape
    choices_row = routes.shape[1]
    experts = lax.axis_size("ep")
    capacity = 2 * tok_rows * choices_row // experts
    recv_rows = experts * capacity
    slot_ids = slot_index(routes, experts, capacity)
    send_w = jnp.zeros((recv_rows,), f32).at[slot_ids].set(route_weight.reshape(-1))
    send_x = (
        jnp.zeros((recv_rows, model_width), jnp.bfloat16)
        .at[slot_ids]
        .set(jnp.repeat(tokens, choices_row, axis=0))
    )
    send_dy = (
        jnp.zeros((recv_rows, model_width), jnp.bfloat16)
        .at[slot_ids]
        .set(jnp.repeat(cotangent, choices_row, axis=0))
    )
    got_x = lax.all_to_all(
        send_x.reshape(experts, capacity, model_width),
        "ep",
        split_axis=0,
        concat_axis=0,
        tiled=True,
    )
    got_dy, got_w = (
        lax.all_to_all(
            send_dy.reshape(experts, capacity, model_width),
            "ep",
            split_axis=0,
            concat_axis=0,
            tiled=True,
        ),
        lax.all_to_all(
            send_w.reshape(experts, capacity, 1).astype(jnp.bfloat16),
            "ep",
            split_axis=0,
            concat_axis=0,
            tiled=True,
        ).astype(jnp.float32),
    )
    rows_x = got_x.reshape(recv_rows, model_width)
    rows_dy = got_dy.reshape(recv_rows, model_width)
    rows_w = got_w.reshape(recv_rows)
    gate_w = w_gate[0]
    up_w = w_up[0]
    down_w = w_down[0]
    gate_pre = jnp.dot(rows_x, gate_w, preferred_element_type=f32)
    up_pre = jnp.dot(rows_x, up_w, preferred_element_type=f32)
    gate_sig = jax.nn.sigmoid(gate_pre)
    act_full = gate_pre * gate_sig * up_pre
    act = act_full.astype(jnp.bfloat16)
    back_hidden = jnp.einsum("rd,fd->rf", rows_dy, down_w, preferred_element_type=f32)
    weighted_cot = (rows_w[:, None] * rows_dy.astype(f32)).astype(jnp.bfloat16)
    d_hidden = rows_w[:, None] * back_hidden
    d_gate = (d_hidden * up_pre * gate_sig * (1.0 + gate_pre * (1.0 - gate_sig))).astype(
        jnp.bfloat16
    )
    d_up = (d_hidden * gate_pre * gate_sig).astype(jnp.bfloat16)
    gate_part = jnp.sum(act_full * back_hidden, axis=1)
    token_part = jnp.einsum("rf,df->rd", d_gate, gate_w, preferred_element_type=f32)
    token_part = token_part + jnp.einsum("rf,df->rd", d_up, up_w, preferred_element_type=f32)
    grad_gate = jnp.einsum("rd,rf->df", rows_x, d_gate, preferred_element_type=f32)[None]
    grad_up = jnp.einsum("rd,rf->df", rows_x, d_up, preferred_element_type=f32)[None]
    grad_down = jnp.einsum("rf,rd->fd", act, weighted_cot, preferred_element_type=f32)[None]
    rounded_part = token_part.astype(jnp.bfloat16).astype(f32)
    shares = lax.psum_scatter(
        rounded_part.astype(jnp.bfloat16), "tp", scatter_dimension=1, tiled=True
    )
    gate_total = lax.psum(gate_part, "tp")
    back_x, back_gate = (
        lax.all_to_all(
            shares.reshape(experts, capacity, -1), "ep", split_axis=0, concat_axis=0, tiled=True
        ),
        lax.all_to_all(
            gate_total.reshape(experts, capacity).astype(jnp.bfloat16),
            "ep",
            split_axis=0,
            concat_axis=0,
            tiled=True,
        ).astype(jnp.float32),
    )
    picked = back_x.reshape(recv_rows, -1)[slot_ids].astype(f32).reshape(tok_rows, choices_row, -1)
    grad_route_weight = back_gate.reshape(recv_rows)[slot_ids].reshape(tok_rows, choices_row)
    grad_tokens = jnp.sum(picked, axis=1).astype(jnp.bfloat16)
    return (grad_tokens, grad_route_weight, grad_gate, grad_up, grad_down)


def kernel(ep, tp, tokens, cotangent, routes_in, weight_in, w_gate, w_up, w_down,
           result, out_home, g_gate, g_up, g_down,
           full, in_v, down_v, weights, part, other, top, bottom,
           in_top, in_bottom, last_top, last_bottom, share, arrived, early,
           d_in, act_w, score, score_rows, scores, total, home, routes, route_weight,
           local, sent, got):
    f32, bf16 = jnp.float32, jnp.bfloat16
    rows, width = tokens.shape
    cols = width // tp
    half = rows // 2
    nz = ep // 2
    e, t = lax.axis_index("ep"), lax.axis_index("tp")
    z, c = e // 2, lax.rem(e, 2)
    y, x = t // 2, lax.rem(t, 2)
    side = z * 2 + 1 - c
    tx, ty = y * 2 + 1 - x, (1 - y) * 2 + x
    td = (1 - y) * 2 + 1 - x
    onward = jnp.where(z < nz // 2, 1, -1)
    middle = jnp.logical_and(z > 0, z < nz - 1)
    outer = jnp.logical_not(middle)
    ahead, behind = z + onward, z - jnp.where(middle, onward, -onward)
    back = [z, ahead, z + 2 * onward, z + jnp.where(middle, -1, 3) * onward]
    groups = {name: i for i, name in enumerate(
        ("pair", "plane", "side", "own", "hand", "quarters", "home", "small", "relay", "relay_w"))}
    names = {}

    def slot(name, count=1):
        if name not in names:
            names[name] = sum(n for _, n in names.values()), count
        return names[name][0]

    def plan(group, src, dst, slot_at, to_e, to_t):
        return pltpu.make_async_remote_copy(
            src_ref=src, dst_ref=dst, send_sem=sent.at[groups[group]], recv_sem=got.at[slot_at],
            device_id={"ep": to_e, "tp": to_t}, device_id_type=pl.DeviceIdType.MESH)

    def push(*args):
        plan(*args).start()

    def drained(group, ref):
        pltpu.make_async_remote_copy(
            src_ref=ref, dst_ref=ref, send_sem=sent.at[groups[group]], recv_sem=got.at[0],
            device_id={"ep": side, "tp": t}, device_id_type=pl.DeviceIdType.MESH).wait_send()

    def landing(dst, slot_at):
        return pltpu.make_async_remote_copy(
            src_ref=dst, dst_ref=dst, send_sem=sent.at[0], recv_sem=got.at[slot_at],
            device_id={"ep": side, "tp": t}, device_id_type=pl.DeviceIdType.MESH)

    def landed(dst, slot_at):
        landing(dst, slot_at).wait_recv()

    barrier = pltpu.get_barrier_semaphore()

    def greet(to_e, to_t):
        pl.semaphore_signal(barrier, inc=1, device_id={"ep": to_e, "tp": to_t},
                            device_id_type=pl.DeviceIdType.MESH)

    for a, turn in ((0, 0), (1, 0), (1, 3), (0, 1), (0, 2), (0, 3), (1, 1), (1, 2)):
        q = (t, tx, ty, td)[turn]
        ref = (tokens, cotangent)[a]
        pltpu.make_async_copy(
            ref.at[:, pl.ds(pl.multiple_of(q * cols, cols), cols)], full.at[e, a, q],
            local.at[(a if turn in (0, 3 * a) else 5 + a)]).start()
    small = [pltpu.make_async_copy(src, dst, local.at[7 + i])
             for i, (src, dst) in enumerate(((routes_in, routes), (weight_in, route_weight)))]
    for copy in small:
        copy.start()
    greet(ahead * 2 + c, t)
    pl.when(middle)(lambda: greet(behind * 2 + c, t))
    greet(e, tx)
    greet(e, ty)
    greet(side, t)

    for name, count in (("along", 6 * nz), ("x", 9), ("y", 9), ("dx", 3), ("dy", 3), ("side", 4), ("side_w", 4),
                        ("pair", 4), ("pairs", 4), ("top", 3), ("tops", 3), ("bottom", 3), ("bottoms", 3),
                        ("last_top", 3), ("last_bottom", 3), ("early", 1), ("share", 1), ("score", 1), ("home", 1)):
        slot(name, count)

    def summed(name, dz):
        return slot(name) + max(dz - 1, 0)

    pl.semaphore_wait(barrier, jnp.where(middle, 5, 4))

    def pieces(s):
        return (full.at[s, 0, t, :half], full.at[s, 0, t, half:], full.at[s, 1, t, :half], full.at[s, 1, t, half:],
                full.at[s, 1, td], weights.at[s])

    def along(block, k):
        return slot("along") + block * 6 + k

    def loaded(ref, i):
        pltpu.make_async_copy(ref, ref, local.at[i]).wait()

    for k, piece in enumerate(pieces(e)):
        if k == 0:
            loaded(full.at[e, 0, 0], 0)
        elif k == 2:
            loaded(full.at[e, 1, pl.ds(0, 2)], 1)
        elif k == 5:
            for copy in small:
                copy.wait()
            named = lax.broadcasted_iota(jnp.int32, (ep, rows), 0)
            hits = [named == routes[pl.ds(i, 1), :] for i in range(routes.shape[0])]
            weights[e] = sum(jnp.where(hit, route_weight[pl.ds(i, 1), :], 0.0) for i, hit in enumerate(hits))
        push("small" if k == 5 else "own", piece, piece, along(z, k), ahead * 2 + c, t)
        copy = plan("relay_w" if k == 5 else "relay", piece, piece, along(z, k), behind * 2 + c, t)
        pl.when(middle)(copy.start)
    hidden = down_v.shape[0]
    loaded(full.at[e, 0, pl.ds(0, 3)], 5)
    loaded(full.at[e, 1, pl.ds(0, 2)], 6)
    loads = [pltpu.make_async_copy(src.at[0], dst, local.at[1 + i]) for i, (src, dst) in enumerate((
        (w_gate, in_v.at[:, pl.ds(0, hidden)]), (w_up, in_v.at[:, pl.ds(hidden, hidden)]), (w_down, down_v)), 1)]
    for copy in loads:
        copy.start()

    @pl.when(outer)
    def _():
        early[...] = jnp.zeros_like(early)

    def own():
        push("small", weights.at[e], weights.at[e], slot("side_w"), side, t)
        push("side", full.at[e], full.at[e], slot("side"), side, t)
        for copy in loads:
            copy.wait()

    onto = {}

    def step(dz, k):
        block = back[dz]
        s = block * 2 + c
        piece = pieces(s)[k]
        landed(piece, along(block, k))
        if dz in onto and dz > 1:
            push("relay_w" if k == 5 else "relay", piece, piece, along(block, k), onto[dz] * 2 + c, t)
        if k < 4:
            to = dz * 3 - 3 + min(k, 2)
            push("plane", piece, piece, slot("x") + to, e, tx)
            push("plane", piece, piece, slot("y") + to, e, ty)
        if k == 5:
            push("small", piece, piece, slot("side_w") + dz, side, t)
        elif k % 2 or k == 4:
            whole = {1: full.at[s, 0, t], 3: full.at[s, 1, t], 4: piece}[k]
            push("side", whole, whole, slot("side") + dz, side, t)
        if k == 4:
            step(dz, 5)

    def near(k):
        step(1, k)

    def pass_on(k):
        for i in (4, 5) if k == 4 else (k,):
            piece = pieces(back[1] * 2 + c)[i]
            push("relay_w" if i == 5 else "relay", piece, piece, along(back[1], i), behind * 2 + c, t)

    def far(k):
        step(2, k)

    def last(k):
        step(3, k)

    def aside(dz, a, q):
        piece = full.at[back[dz] * 2 + c, a, q]
        push("side", piece, piece, slot("side") + dz, side, t)

    def relayx(dz):
        piece = full.at[back[dz] * 2 + c, 0, ty, :half]
        landed(piece, slot("y") + dz * 3 - 3)
        push("quarters", piece, piece, slot("dx") + dz - 1, e, tx)

    def relayy(dz):
        s = back[dz] * 2 + c
        piece = full.at[s, 0, tx, half:]
        landed(piece, slot("x") + dz * 3 - 2)
        push("quarters", piece, piece, slot("dy") + dz - 1, e, ty)
        landed(full.at[s, 0, ty, half:], slot("y") + dz * 3 - 2)
        aside(dz, 0, ty)
        landed(full.at[s, 0, tx, :half], slot("x") + dz * 3 - 3)
        aside(dz, 0, tx)

    def crossed(dz):
        s = back[dz] * 2 + c
        landed(full.at[s, 1, ty], slot("y") + dz * 3 - 1)
        aside(dz, 1, ty)
        landed(full.at[s, 1, tx], slot("x") + dz * 3 - 1)
        aside(dz, 1, tx)

    def diag(dz):
        s = back[dz] * 2 + c
        landed(full.at[s, 0, td, :half], slot("dx") + dz - 1)
        landed(full.at[s, 0, td, half:], slot("dy") + dz - 1)
        aside(dz, 0, td)

    def nt(a, b):
        return lax.dot_general(a, b, (((1,), (1,)), ((), ())), preferred_element_type=f32)

    def tn(a, b):
        return lax.dot_general(a, b, (((0,), (0,)), ((), ())), preferred_element_type=f32)

    def column(block):
        mine = lax.broadcasted_iota(jnp.int32, (ep, rows), 0) == e
        row = jnp.sum(jnp.where(mine, weights[block], 0.0), axis=0, keepdims=True)
        return jnp.transpose(jnp.broadcast_to(row, (rows, rows)))[:, :1]

    def fwd(dz):
        b = back[dz] * 2
        landed(full.at[b + 1 - c], slot("side") + dz)
        landed(weights.at[b + 1 - c], slot("side_w") + dz)
        gu = bk = None
        for q in range(tp):
            span = pl.ds(q * cols, cols)
            xs = jnp.concatenate([full[b, 0, q], full[b + 1, 0, q]], axis=0)
            dy = jnp.concatenate([full[b, 1, q], full[b + 1, 1, q]], axis=0)
            gu_q = jnp.dot(xs, in_v[span, :], preferred_element_type=f32)
            b_q = nt(dy, down_v[:, span])
            gu, bk = (gu_q, b_q) if q == 0 else (gu + gu_q, bk + b_q)
        g, u = gu[:, :hidden], gu[:, hidden:]
        w = jnp.concatenate([column(b), column(b + 1)], axis=0)
        sig = jax.nn.sigmoid(g)
        silu = g * sig
        act = silu * u
        d_h = w * bk
        dg = (d_h * u * sig * (1.0 + g * (1.0 - sig))).astype(bf16)
        du = (d_h * silu).astype(bf16)
        aw = (w * act).astype(bf16)
        sums = jnp.sum(act * bk, axis=1, keepdims=True)
        for i in range(2):
            cut = slice(i * rows, (i + 1) * rows)
            d_in[b + i, :, :hidden] = dg[cut]
            d_in[b + i, :, hidden:] = du[cut]
            act_w[b + i] = aw[cut]
            score[b + i] = jnp.transpose(jnp.broadcast_to(sums[cut], (rows, rows)))[:8]

    def bwd(dz):
        b = back[dz] * 2
        d = jnp.concatenate([d_in[b], d_in[b + 1]], axis=0)
        for group, name in (((td,), "pair"), ((tx, ty, t), "pairs")):
            for q in group:
                piece = nt(d, in_v[pl.ds(pl.multiple_of(q * cols, cols), cols), :]).astype(bf16)
                part[b, q] = piece[:rows]
                part[b + 1, q] = piece[rows:]
            for q in group:
                push("pair", part.at[b + 1 - c, q], other.at[dz, q], slot(name) + dz, side, t)

    def add(*terms):
        value = terms[0].astype(f32)
        for term in terms[1:]:
            value = value + term.astype(f32)
        return value

    def paired(dz, q, cut=slice(None)):
        terms = [part[back[dz] * 2 + c, q, cut], other[dz, q, cut]]
        return add(*terms, *([early[0, q, cut], early[1, q, cut]] if dz == 0 else [])).astype(bf16)

    upper, lower = slice(0, half), slice(half, rows)

    def hand(dz):
        landed(other.at[dz, td], slot("pair") + dz)
        landed(other.at[dz, pl.ds(0, 3)], slot("pairs") + dz)
        s = back[dz] * 2 + c
        for q in range(tp):
            part[s, q] = paired(dz, q)
            push("hand", part.at[s, q], early.at[jnp.where(middle, 1, 0), q], slot("early"), ahead * 2 + c, t)

    def first(dz):
        landed(other.at[dz, td], slot("pair") + dz)
        if dz == 0:
            if onto:
                landed(early, slot("early"))
        top[dz, 3] = paired(dz, td, upper)
        push("quarters", top.at[dz, 3], in_top.at[dz, 1], summed("top", dz), e, tx)
        bottom[dz, 3] = paired(dz, td, lower)
        push("quarters", bottom.at[dz, 3], in_bottom.at[dz, 1], summed("bottom", dz), e, ty)

    def firstB(dz):
        landed(other.at[dz, pl.ds(0, 3)], slot("pairs") + dz)
        top[dz, 2] = paired(dz, tx, upper)
        push("quarters", top.at[dz, 2], in_top.at[dz, 0], summed("tops", dz), e, tx)
        bottom[dz, 2] = paired(dz, ty, lower)
        push("quarters", bottom.at[dz, 2], in_bottom.at[dz, 0], summed("bottoms", dz), e, ty)
        top[dz, 1] = paired(dz, ty, upper)
        bottom[dz, 1] = paired(dz, tx, lower)
        top[dz, 0] = paired(dz, t, upper)
        bottom[dz, 0] = paired(dz, t, lower)

    def second(dz):
        landed(in_top.at[dz, 1], summed("top", dz))
        top[dz, 1] = add(top[dz, 1], in_top[dz, 1]).astype(bf16)
        push("quarters", top.at[dz, 1], last_top.at[dz], summed("last_top", dz), e, ty)
        landed(in_bottom.at[dz, 1], summed("bottom", dz))
        bottom[dz, 1] = add(bottom[dz, 1], in_bottom[dz, 1]).astype(bf16)
        push("quarters", bottom.at[dz, 1], last_bottom.at[dz], summed("last_bottom", dz), e, tx)

    kept = []

    def third(dz):
        for cut, mine, got_in, ending, name in (
                (pl.ds(0, half), top, in_top, last_top, "top"), (pl.ds(half, half), bottom, in_bottom, last_bottom, "bottom")):
            landed(got_in.at[dz, 0], summed(name + "s", dz))
            landed(ending.at[dz], summed("last_" + name, dz))
            value = add(mine[dz, 0], got_in[dz, 0], ending[dz])
            if dz:
                share[dz - 2, cut] = value.astype(bf16)
                push("quarters", share.at[dz - 2, cut], arrived.at[z, cut], slot("share"), back[dz] * 2 + c, t)
            else:
                kept.append(value)

    def wg(i):
        if i < 3:
            right = d_in[...].reshape(ep * rows, 2 * hidden)
            for q in range(i * 2 - 2, i * 2):
                both = tn(full[:, 0, q].reshape(ep * rows, cols), right)
                g_gate[0, pl.ds(q * cols, cols), :] = both[:, :hidden]
                g_up[0, pl.ds(q * cols, cols), :] = both[:, hidden:]
        else:
            left = act_w[...].reshape(ep * rows, hidden)
            for q in range(tp):
                g_down[0, :, pl.ds(q * cols, cols)] = tn(left, full[:, 1, q].reshape(ep * rows, cols))

    def tally():
        score_rows[...] = jnp.concatenate([score[j, :1] for j in range(ep)], axis=0)
        for k in range(1, tp):
            push("small", score_rows, scores.at[t], slot("score"), e, lax.rem(t + k, tp))
        scores[t] = score_rows[...]

    def homeward():
        landed(scores.at[pl.ds(0, tp - 1)], slot("score"))
        total[...] = add(*[scores[j] for j in range(tp)])
        for k in range(1, ep):
            push("home", total, home.at[e], slot("home"), lax.rem(e + k, ep), t)
        home[e] = total[...]

    def finish(count, blocks):
        landed(arrived.at[pl.ds(0, count)], slot("share"))
        for cut, value in zip((upper, lower), kept):
            result[cut] = add(value, *[arrived[back[i], cut] for i in blocks]).astype(bf16)
        kept.clear()

    @pl.when(outer)
    def _():
        for act, *where in (
            (near, 0), (own,), (near, 1), (relayx, 1), (near, 2), (near, 3), (fwd, 0), (relayy, 1), (far, 0),
            (far, 1), (far, 2), (diag, 1), (near, 4), (crossed, 1), (last, 0), (far, 3), (fwd, 1), (relayx, 2),
            (relayy, 2), (last, 1), (bwd, 1), (hand, 1), (crossed, 2), (relayx, 3), (diag, 2), (last, 2), (far, 4),
            (relayy, 3), (fwd, 2), (last, 3), (bwd, 2), (first, 2), (last, 4), (crossed, 3), (diag, 3), (firstB, 2),
            (bwd, 0), (second, 2), (fwd, 3), (first, 0), (bwd, 3), (tally,), (first, 3), (third, 2), (firstB, 3),
            (second, 3), (wg, 2), (firstB, 0), (second, 0), (wg, 3), (third, 3), (homeward,), (wg, 1), (third, 0),
        ):
            with jax.named_scope(act.__name__):
                act(*where)
        finish(nz - 1, (1, 2, 3))

    @pl.when(middle)
    def _():
        onto.update({2: behind, 3: ahead})
        for act, *where in (
            (last, 0), (near, 0), (own,), (near, 1), (pass_on, 0), (last, 1), (near, 2), (relayx, 1), (near, 3),
            (pass_on, 1), (relayy, 1), (relayx, 3), (pass_on, 2), (last, 2), (far, 0), (pass_on, 3), (relayy, 3),
            (last, 3), (far, 1), (near, 4), (diag, 1), (far, 2), (crossed, 1), (last, 4), (pass_on, 4), (far, 3),
            (fwd, 1), (bwd, 1), (hand, 1), (crossed, 3), (diag, 3), (far, 4), (fwd, 0), (relayx, 2), (relayy, 2),
            (fwd, 3), (bwd, 3), (first, 3), (crossed, 2), (diag, 2), (firstB, 3), (fwd, 2), (second, 3), (bwd, 2),
            (first, 2), (bwd, 0), (tally,), (third, 3), (firstB, 2), (second, 2), (first, 0), (firstB, 0), (wg, 2),
            (third, 2), (second, 0), (wg, 3), (homeward,), (wg, 1), (third, 0),
        ):
            with jax.named_scope(act.__name__):
                act(*where)
        finish(1, (2,))

    landed(home.at[pl.ds(0, ep - 1)], slot("home"))
    back_home = jnp.concatenate(
        [jnp.sum(jnp.where(named == e, home[j], 0.0), axis=0, keepdims=True) for j in range(ep)], axis=0)
    for k, hit in enumerate(hits):
        out_home[pl.ds(k, 1), :] = jnp.sum(jnp.where(hit, back_home, 0.0), axis=0, keepdims=True)
    assert sum(n for _, n in names.values()) == got.shape[0]
    drained("pair", other)
    drained("plane", full.at[pl.ds(0, 3), 0])
    drained("side", full.at[pl.ds(0, 4)])
    drained("own", full.at[0, 0, pl.ds(0, 3)])
    drained("hand", full.at[0, 0])
    drained("quarters", full.at[pl.ds(0, 7), 0, pl.ds(0, 2)])
    drained("home", weights.at[pl.ds(0, ep - 1)])
    drained("small", weights)

    @pl.when(middle)
    def _():
        drained("relay", full.at[pl.ds(0, 3), 0])
        drained("relay_w", weights.at[pl.ds(0, 4)])


def deliver(*refs):
    half = (len(refs) - 1) // 2
    copies = [pltpu.make_async_copy(src, dst, refs[-1].at[i])
              for i, (src, dst) in enumerate(zip(refs[:half], refs[half:-1]))]
    for copy in copies:
        copy.start()
    for copy in copies:
        copy.wait()


def dense(tokens, cotangent, routes, route_weight, w_gate, w_up, w_down):
    f32, bf16 = jnp.float32, jnp.bfloat16
    rows, width = tokens.shape
    ep, tp = lax.axis_size("ep"), lax.axis_size("tp")
    cols, half, nz, hidden = width // tp, rows // 2, ep // 2, w_gate.shape[2]
    anywhere, near = pl.BlockSpec(memory_space=pltpu.HBM), pl.BlockSpec(memory_space=pltpu.VMEM)

    def held(space, *arrays):
        return [pltpu.with_memory_space_constraint(x, space) for x in arrays]

    shapes = ((rows, cols), bf16), (routes.T.shape, f32), (w_gate.shape, f32), (w_up.shape, f32), (w_down.shape, f32)
    parts = pl.pallas_call(
        functools.partial(kernel, ep, tp),
        out_shape=tuple(pltpu.VMEM(*shape) for shape in shapes),
        in_specs=[anywhere] * 7,
        out_specs=(near,) * 5,
        scratch_shapes=[
            pltpu.VMEM((ep, 2, tp, rows, cols), bf16),
            pltpu.VMEM((width, 2 * hidden), bf16),
            pltpu.VMEM((hidden, width), bf16),
            pltpu.VMEM((ep, ep, rows), f32),
            pltpu.VMEM((ep, tp, rows, cols), bf16),
            pltpu.VMEM((nz, tp, rows, cols), bf16),
            pltpu.VMEM((nz, 4, half, cols), bf16),
            pltpu.VMEM((nz, 4, half, cols), bf16),
            pltpu.VMEM((nz, 2, half, cols), bf16),
            pltpu.VMEM((nz, 2, half, cols), bf16),
            pltpu.VMEM((nz, half, cols), bf16),
            pltpu.VMEM((nz, half, cols), bf16),
            pltpu.VMEM((2, rows, cols), bf16),
            pltpu.VMEM((nz, rows, cols), bf16),
            pltpu.VMEM((2, tp, rows, cols), bf16),
            pltpu.VMEM((ep, rows, 2 * hidden), bf16),
            pltpu.VMEM((ep, rows, hidden), bf16),
            pltpu.VMEM((ep, 8, rows), f32),
            pltpu.VMEM((ep, rows), f32),
            pltpu.VMEM((tp, ep, rows), f32),
            pltpu.VMEM((ep, rows), f32),
            pltpu.VMEM((ep, ep, rows), f32),
            pltpu.VMEM(routes.T.shape, routes.dtype),
            pltpu.VMEM(routes.T.shape, f32),
            pltpu.SemaphoreType.DMA((9,)),
            pltpu.SemaphoreType.DMA((10,)),
            pltpu.SemaphoreType.DMA((86,)),
        ],
        compiler_params=pltpu.CompilerParams(
            collective_id=0, has_side_effects=True, vmem_limit_bytes=50 * 1024 * 1024),
    )(*held(pltpu.HBM, tokens, cotangent, routes.T, route_weight.T, w_gate, w_up, w_down))
    grad_tokens, grw, *grads = pl.pallas_call(
        deliver,
        out_shape=tuple(jax.ShapeDtypeStruct(*shape) for shape in shapes),
        in_specs=[near] * 5,
        out_specs=(anywhere,) * 5,
        scratch_shapes=[pltpu.SemaphoreType.DMA((5,))],
        compiler_params=pltpu.CompilerParams(vmem_limit_bytes=1 << 20),
    )(*held(pltpu.VMEM, *parts))
    return grad_tokens, grw.T, *grads


def on_device(*args):
    rows, width = args[0].shape
    ep, tp = lax.axis_size("ep"), lax.axis_size("tp")
    fits = tp == 4 and ep == 8 and rows % 128 == 0 and 4 * rows * width * ep <= 1 << 24
    return (dense if fits else slotted)(*args)


def solution(mesh):
    return jax.shard_map(
        on_device,
        mesh=mesh,
        in_specs=(
            P("ep", None),
            P("ep", None),
            P("ep", None),
            P("ep", None),
            P("ep", None, "tp"),
            P("ep", None, "tp"),
            P("ep", "tp", None),
        ),
        out_specs=(
            P("ep", "tp"),
            P("ep", None),
            P("ep", None, "tp"),
            P("ep", None, "tp"),
            P("ep", "tp", None),
        ),
        check_vma=False,
    )
```

```python
import functools

import jax
import jax.numpy as jnp
from jax import lax
from jax.experimental import pallas as pl
from jax.experimental.pallas import tpu as pltpu
from jax.sharding import PartitionSpec as P


def slot_index(block_routes, experts, capacity):
    flat_ids = block_routes.reshape(-1)
    onehot = (flat_ids[:, None] == jnp.arange(experts, dtype=jnp.int32)[None, :]).astype(jnp.int32)
    earlier = jnp.cumsum(onehot, axis=0) - onehot
    return flat_ids * capacity + jnp.sum(earlier * onehot, axis=1)


def slotted(tokens, cotangent, routes, route_weight, w_gate, w_up, w_down):
    f32 = jnp.float32
    tok_rows, model_width = tokens.shape
    choices_row = routes.shape[1]
    experts = lax.axis_size("ep")
    capacity = 2 * tok_rows * choices_row // experts
    recv_rows = experts * capacity
    slot_ids = slot_index(routes, experts, capacity)
    send_w = jnp.zeros((recv_rows,), f32).at[slot_ids].set(route_weight.reshape(-1))
    send_x = (
        jnp.zeros((recv_rows, model_width), jnp.bfloat16)
        .at[slot_ids]
        .set(jnp.repeat(tokens, choices_row, axis=0))
    )
    send_dy = (
        jnp.zeros((recv_rows, model_width), jnp.bfloat16)
        .at[slot_ids]
        .set(jnp.repeat(cotangent, choices_row, axis=0))
    )
    got_x = lax.all_to_all(
        send_x.reshape(experts, capacity, model_width),
        "ep",
        split_axis=0,
        concat_axis=0,
        tiled=True,
    )
    got_dy, got_w = (
        lax.all_to_all(
            send_dy.reshape(experts, capacity, model_width),
            "ep",
            split_axis=0,
            concat_axis=0,
            tiled=True,
        ),
        lax.all_to_all(
            send_w.reshape(experts, capacity, 1).astype(jnp.bfloat16),
            "ep",
            split_axis=0,
            concat_axis=0,
            tiled=True,
        ).astype(jnp.float32),
    )
    rows_x = got_x.reshape(recv_rows, model_width)
    rows_dy = got_dy.reshape(recv_rows, model_width)
    rows_w = got_w.reshape(recv_rows)
    gate_w = w_gate[0]
    up_w = w_up[0]
    down_w = w_down[0]
    gate_pre = jnp.dot(rows_x, gate_w, preferred_element_type=f32)
    up_pre = jnp.dot(rows_x, up_w, preferred_element_type=f32)
    gate_sig = jax.nn.sigmoid(gate_pre)
    act_full = gate_pre * gate_sig * up_pre
    act = act_full.astype(jnp.bfloat16)
    back_hidden = jnp.einsum("rd,fd->rf", rows_dy, down_w, preferred_element_type=f32)
    weighted_cot = (rows_w[:, None] * rows_dy.astype(f32)).astype(jnp.bfloat16)
    d_hidden = rows_w[:, None] * back_hidden
    d_gate = (d_hidden * up_pre * gate_sig * (1.0 + gate_pre * (1.0 - gate_sig))).astype(
        jnp.bfloat16
    )
    d_up = (d_hidden * gate_pre * gate_sig).astype(jnp.bfloat16)
    gate_part = jnp.sum(act_full * back_hidden, axis=1)
    token_part = jnp.einsum("rf,df->rd", d_gate, gate_w, preferred_element_type=f32)
    token_part = token_part + jnp.einsum("rf,df->rd", d_up, up_w, preferred_element_type=f32)
    grad_gate = jnp.einsum("rd,rf->df", rows_x, d_gate, preferred_element_type=f32)[None]
    grad_up = jnp.einsum("rd,rf->df", rows_x, d_up, preferred_element_type=f32)[None]
    grad_down = jnp.einsum("rf,rd->fd", act, weighted_cot, preferred_element_type=f32)[None]
    rounded_part = token_part.astype(jnp.bfloat16).astype(f32)
    shares = lax.psum_scatter(
        rounded_part.astype(jnp.bfloat16), "tp", scatter_dimension=1, tiled=True
    )
    gate_total = lax.psum(gate_part, "tp")
    back_x, back_gate = (
        lax.all_to_all(
            shares.reshape(experts, capacity, -1), "ep", split_axis=0, concat_axis=0, tiled=True
        ),
        lax.all_to_all(
            gate_total.reshape(experts, capacity).astype(jnp.bfloat16),
            "ep",
            split_axis=0,
            concat_axis=0,
            tiled=True,
        ).astype(jnp.float32),
    )
    picked = back_x.reshape(recv_rows, -1)[slot_ids].astype(f32).reshape(tok_rows, choices_row, -1)
    grad_route_weight = back_gate.reshape(recv_rows)[slot_ids].reshape(tok_rows, choices_row)
    grad_tokens = jnp.sum(picked, axis=1).astype(jnp.bfloat16)
    return (grad_tokens, grad_route_weight, grad_gate, grad_up, grad_down)


def kernel(ep, tp, tokens, cotangent, routes_in, weight_in, w_gate, w_up, w_down,
           result, out_home, g_gate, g_up, g_down,
           full, in_v, down_v, weights, part, other, top, bottom,
           in_top, in_bottom, last_top, last_bottom, share, arrived, early,
           d_in, act_w, score, score_rows, scores, total, home, routes, route_weight,
           local, sent, got):
    f32, bf16 = jnp.float32, jnp.bfloat16
    rows, width = tokens.shape
    cols = width // tp
    half = rows // 2
    nz = ep // 2
    e, t = lax.axis_index("ep"), lax.axis_index("tp")
    z, c = e // 2, lax.rem(e, 2)
    y, x = t // 2, lax.rem(t, 2)
    side = z * 2 + 1 - c
    tx, ty = y * 2 + 1 - x, (1 - y) * 2 + x
    td = (1 - y) * 2 + 1 - x
    onward = jnp.where(z < nz // 2, 1, -1)
    middle = jnp.logical_and(z > 0, z < nz - 1)
    outer = jnp.logical_not(middle)
    ahead, behind = z + onward, z - jnp.where(middle, onward, -onward)
    back = [z, ahead, z + 2 * onward, z + jnp.where(middle, -1, 3) * onward]
    groups = {name: i for i, name in enumerate(
        ("pair", "plane", "side", "own", "hand", "quarters", "home", "small", "relay", "relay_w"))}
    names = {}

    def slot(name, count=1):
        if name not in names:
            names[name] = sum(n for _, n in names.values()), count
        return names[name][0]

    def plan(group, src, dst, slot_at, to_e, to_t):
        return pltpu.make_async_remote_copy(
            src_ref=src, dst_ref=dst, send_sem=sent.at[groups[group]], recv_sem=got.at[slot_at],
            device_id={"ep": to_e, "tp": to_t}, device_id_type=pl.DeviceIdType.MESH)

    def push(*args):
        plan(*args).start()

    def drained(group, ref):
        pltpu.make_async_remote_copy(
            src_ref=ref, dst_ref=ref, send_sem=sent.at[groups[group]], recv_sem=got.at[0],
            device_id={"ep": side, "tp": t}, device_id_type=pl.DeviceIdType.MESH).wait_send()

    def landing(dst, slot_at):
        return pltpu.make_async_remote_copy(
            src_ref=dst, dst_ref=dst, send_sem=sent.at[0], recv_sem=got.at[slot_at],
            device_id={"ep": side, "tp": t}, device_id_type=pl.DeviceIdType.MESH)

    def landed(dst, slot_at):
        landing(dst, slot_at).wait_recv()

    barrier = pltpu.get_barrier_semaphore()

    def greet(to_e, to_t):
        pl.semaphore_signal(barrier, inc=1, device_id={"ep": to_e, "tp": to_t},
                            device_id_type=pl.DeviceIdType.MESH)

    for a, turn in ((0, 0), (1, 0), (1, 3), (0, 1), (0, 2), (0, 3), (1, 1), (1, 2)):
        q = (t, tx, ty, td)[turn]
        ref = (tokens, cotangent)[a]
        pltpu.make_async_copy(
            ref.at[:, pl.ds(pl.multiple_of(q * cols, cols), cols)], full.at[e, a, q],
            local.at[(a if turn in (0, 3 * a) else 5 + a)]).start()
    small = [pltpu.make_async_copy(src, dst, local.at[7 + i])
             for i, (src, dst) in enumerate(((routes_in, routes), (weight_in, route_weight)))]
    for copy in small:
        copy.start()
    greet(ahead * 2 + c, t)
    pl.when(middle)(lambda: greet(behind * 2 + c, t))
    greet(e, tx)
    greet(e, ty)
    greet(side, t)

    for name, count in (("along", 6 * nz), ("x", 9), ("y", 9), ("dx", 3), ("dy", 3), ("side", 4), ("side_w", 4),
                        ("pair", 4), ("pairs", 4), ("top", 3), ("tops", 3), ("bottom", 3), ("bottoms", 3),
                        ("last_top", 3), ("last_bottom", 3), ("early", 1), ("share", 1), ("score", 1), ("home", 1)):
        slot(name, count)

    def summed(name, dz):
        return slot(name) + max(dz - 1, 0)

    pl.semaphore_wait(barrier, jnp.where(middle, 5, 4))

    def pieces(s):
        return (full.at[s, 0, t, :half], full.at[s, 0, t, half:], full.at[s, 1, t, :half], full.at[s, 1, t, half:],
                full.at[s, 1, td], weights.at[s])

    def along(block, k):
        return slot("along") + block * 6 + k

    def loaded(ref, i):
        pltpu.make_async_copy(ref, ref, local.at[i]).wait()

    for k, piece in enumerate(pieces(e)):
        if k == 0:
            loaded(full.at[e, 0, 0], 0)
        elif k == 2:
            loaded(full.at[e, 1, pl.ds(0, 2)], 1)
        elif k == 5:
            for copy in small:
                copy.wait()
            named = lax.broadcasted_iota(jnp.int32, (ep, rows), 0)
            hits = [named == routes[pl.ds(i, 1), :] for i in range(routes.shape[0])]
            weights[e] = sum(jnp.where(hit, route_weight[pl.ds(i, 1), :], 0.0) for i, hit in enumerate(hits))
        push("small" if k == 5 else "own", piece, piece, along(z, k), ahead * 2 + c, t)
        copy = plan("relay_w" if k == 5 else "relay", piece, piece, along(z, k), behind * 2 + c, t)
        pl.when(middle)(copy.start)
    hidden = down_v.shape[0]
    loaded(full.at[e, 0, pl.ds(0, 3)], 5)
    loaded(full.at[e, 1, pl.ds(0, 2)], 6)
    loads = [pltpu.make_async_copy(src.at[0], dst, local.at[1 + i]) for i, (src, dst) in enumerate((
        (w_gate, in_v.at[:, pl.ds(0, hidden)]), (w_up, in_v.at[:, pl.ds(hidden, hidden)]), (w_down, down_v)), 1)]
    for copy in loads:
        copy.start()

    @pl.when(outer)
    def _():
        early[...] = jnp.zeros_like(early)

    def own():
        push("small", weights.at[e], weights.at[e], slot("side_w"), side, t)
        push("side", full.at[e], full.at[e], slot("side"), side, t)
        for copy in loads:
            copy.wait()

    onto = {}

    def step(dz, k):
        block = back[dz]
        s = block * 2 + c
        piece = pieces(s)[k]
        landed(piece, along(block, k))
        if dz in onto and dz > 1:
            push("relay_w" if k == 5 else "relay", piece, piece, along(block, k), onto[dz] * 2 + c, t)
        if k < 4:
            to = dz * 3 - 3 + min(k, 2)
            push("plane", piece, piece, slot("x") + to, e, tx)
            push("plane", piece, piece, slot("y") + to, e, ty)
        if k == 5:
            push("small", piece, piece, slot("side_w") + dz, side, t)
        elif k % 2 or k == 4:
            whole = {1: full.at[s, 0, t], 3: full.at[s, 1, t], 4: piece}[k]
            push("side", whole, whole, slot("side") + dz, side, t)
        if k == 4:
            step(dz, 5)

    def near(k):
        step(1, k)

    def pass_on(k):
        for i in (4, 5) if k == 4 else (k,):
            piece = pieces(back[1] * 2 + c)[i]
            push("relay_w" if i == 5 else "relay", piece, piece, along(back[1], i), behind * 2 + c, t)

    def far(k):
        step(2, k)

    def last(k):
        step(3, k)

    def aside(dz, a, q):
        piece = full.at[back[dz] * 2 + c, a, q]
        push("side", piece, piece, slot("side") + dz, side, t)

    def relayx(dz):
        piece = full.at[back[dz] * 2 + c, 0, ty, :half]
        landed(piece, slot("y") + dz * 3 - 3)
        push("quarters", piece, piece, slot("dx") + dz - 1, e, tx)

    def relayy(dz):
        s = back[dz] * 2 + c
        piece = full.at[s, 0, tx, half:]
        landed(piece, slot("x") + dz * 3 - 2)
        push("quarters", piece, piece, slot("dy") + dz - 1, e, ty)
        landed(full.at[s, 0, ty, half:], slot("y") + dz * 3 - 2)
        aside(dz, 0, ty)
        landed(full.at[s, 0, tx, :half], slot("x") + dz * 3 - 3)
        aside(dz, 0, tx)

    def crossed(dz):
        s = back[dz] * 2 + c
        landed(full.at[s, 1, ty], slot("y") + dz * 3 - 1)
        aside(dz, 1, ty)
        landed(full.at[s, 1, tx], slot("x") + dz * 3 - 1)
        aside(dz, 1, tx)

    def diag(dz):
        s = back[dz] * 2 + c
        landed(full.at[s, 0, td, :half], slot("dx") + dz - 1)
        landed(full.at[s, 0, td, half:], slot("dy") + dz - 1)
        aside(dz, 0, td)

    def nt(a, b):
        return lax.dot_general(a, b, (((1,), (1,)), ((), ())), preferred_element_type=f32)

    def tn(a, b):
        return lax.dot_general(a, b, (((0,), (0,)), ((), ())), preferred_element_type=f32)

    def column(block):
        mine = lax.broadcasted_iota(jnp.int32, (ep, rows), 0) == e
        row = jnp.sum(jnp.where(mine, weights[block], 0.0), axis=0, keepdims=True)
        return jnp.transpose(jnp.broadcast_to(row, (rows, rows)))[:, :1]

    def fwd(dz):
        b = back[dz] * 2
        landed(full.at[b + 1 - c], slot("side") + dz)
        landed(weights.at[b + 1 - c], slot("side_w") + dz)
        gu = bk = None
        for q in range(tp):
            span = pl.ds(q * cols, cols)
            xs = jnp.concatenate([full[b, 0, q], full[b + 1, 0, q]], axis=0)
            dy = jnp.concatenate([full[b, 1, q], full[b + 1, 1, q]], axis=0)
            gu_q = jnp.dot(xs, in_v[span, :], preferred_element_type=f32)
            b_q = nt(dy, down_v[:, span])
            gu, bk = (gu_q, b_q) if q == 0 else (gu + gu_q, bk + b_q)
        g, u = gu[:, :hidden], gu[:, hidden:]
        w = jnp.concatenate([column(b), column(b + 1)], axis=0)
        sig = jax.nn.sigmoid(g)
        silu = g * sig
        act = silu * u
        d_h = w * bk
        dg = (d_h * u * sig * (1.0 + g * (1.0 - sig))).astype(bf16)
        du = (d_h * silu).astype(bf16)
        aw = (w * act).astype(bf16)
        sums = jnp.sum(act * bk, axis=1, keepdims=True)
        for i in range(2):
            cut = slice(i * rows, (i + 1) * rows)
            d_in[b + i, :, :hidden] = dg[cut]
            d_in[b + i, :, hidden:] = du[cut]
            act_w[b + i] = aw[cut]
            score[b + i] = jnp.transpose(jnp.broadcast_to(sums[cut], (rows, rows)))[:8]

    def bwd(dz):
        b = back[dz] * 2
        d = jnp.concatenate([d_in[b], d_in[b + 1]], axis=0)
        for group, name in (((td,), "pair"), ((tx, ty, t), "pairs")):
            for q in group:
                piece = nt(d, in_v[pl.ds(pl.multiple_of(q * cols, cols), cols), :]).astype(bf16)
                part[b, q] = piece[:rows]
                part[b + 1, q] = piece[rows:]
            for q in group:
                push("pair", part.at[b + 1 - c, q], other.at[dz, q], slot(name) + dz, side, t)

    def add(*terms):
        value = terms[0].astype(f32)
        for term in terms[1:]:
            value = value + term.astype(f32)
        return value

    def paired(dz, q, cut=slice(None)):
        terms = [part[back[dz] * 2 + c, q, cut], other[dz, q, cut]]
        return add(*terms, *([early[0, q, cut], early[1, q, cut]] if dz == 0 else [])).astype(bf16)

    upper, lower = slice(0, half), slice(half, rows)

    def hand(dz):
        landed(other.at[dz, td], slot("pair") + dz)
        landed(other.at[dz, pl.ds(0, 3)], slot("pairs") + dz)
        s = back[dz] * 2 + c
        for q in range(tp):
            part[s, q] = paired(dz, q)
            push("hand", part.at[s, q], early.at[jnp.where(middle, 1, 0), q], slot("early"), ahead * 2 + c, t)

    def first(dz):
        landed(other.at[dz, td], slot("pair") + dz)
        if dz == 0:
            if onto:
                landed(early, slot("early"))
        top[dz, 3] = paired(dz, td, upper)
        push("quarters", top.at[dz, 3], in_top.at[dz, 1], summed("top", dz), e, tx)
        bottom[dz, 3] = paired(dz, td, lower)
        push("quarters", bottom.at[dz, 3], in_bottom.at[dz, 1], summed("bottom", dz), e, ty)

    def firstB(dz):
        landed(other.at[dz, pl.ds(0, 3)], slot("pairs") + dz)
        top[dz, 2] = paired(dz, tx, upper)
        push("quarters", top.at[dz, 2], in_top.at[dz, 0], summed("tops", dz), e, tx)
        bottom[dz, 2] = paired(dz, ty, lower)
        push("quarters", bottom.at[dz, 2], in_bottom.at[dz, 0], summed("bottoms", dz), e, ty)
        top[dz, 1] = paired(dz, ty, upper)
        bottom[dz, 1] = paired(dz, tx, lower)
        top[dz, 0] = paired(dz, t, upper)
        bottom[dz, 0] = paired(dz, t, lower)

    def second(dz):
        landed(in_top.at[dz, 1], summed("top", dz))
        top[dz, 1] = add(top[dz, 1], in_top[dz, 1]).astype(bf16)
        push("quarters", top.at[dz, 1], last_top.at[dz], summed("last_top", dz), e, ty)
        landed(in_bottom.at[dz, 1], summed("bottom", dz))
        bottom[dz, 1] = add(bottom[dz, 1], in_bottom[dz, 1]).astype(bf16)
        push("quarters", bottom.at[dz, 1], last_bottom.at[dz], summed("last_bottom", dz), e, tx)

    kept = []

    def third(dz):
        for cut, mine, got_in, ending, name in (
                (pl.ds(0, half), top, in_top, last_top, "top"), (pl.ds(half, half), bottom, in_bottom, last_bottom, "bottom")):
            landed(got_in.at[dz, 0], summed(name + "s", dz))
            landed(ending.at[dz], summed("last_" + name, dz))
            value = add(mine[dz, 0], got_in[dz, 0], ending[dz])
            if dz:
                share[dz - 2, cut] = value.astype(bf16)
                push("quarters", share.at[dz - 2, cut], arrived.at[z, cut], slot("share"), back[dz] * 2 + c, t)
            else:
                kept.append(value)

    def wg(i):
        if i < 3:
            right = d_in[...].reshape(ep * rows, 2 * hidden)
            for q in range(i * 2 - 2, i * 2):
                both = tn(full[:, 0, q].reshape(ep * rows, cols), right)
                g_gate[0, pl.ds(q * cols, cols), :] = both[:, :hidden]
                g_up[0, pl.ds(q * cols, cols), :] = both[:, hidden:]
        else:
            left = act_w[...].reshape(ep * rows, hidden)
            for q in range(tp):
                g_down[0, :, pl.ds(q * cols, cols)] = tn(left, full[:, 1, q].reshape(ep * rows, cols))

    def tally():
        score_rows[...] = jnp.concatenate([score[j, :1] for j in range(ep)], axis=0)
        for k in range(1, tp):
            push("small", score_rows, scores.at[t], slot("score"), e, lax.rem(t + k, tp))
        scores[t] = score_rows[...]

    def homeward():
        landed(scores.at[pl.ds(0, tp - 1)], slot("score"))
        total[...] = add(*[scores[j] for j in range(tp)])
        for k in range(1, ep):
            push("home", total, home.at[e], slot("home"), lax.rem(e + k, ep), t)
        home[e] = total[...]

    def finish(count, blocks):
        landed(arrived.at[pl.ds(0, count)], slot("share"))
        for cut, value in zip((upper, lower), kept):
            result[cut] = add(value, *[arrived[back[i], cut] for i in blocks]).astype(bf16)
        kept.clear()

    @pl.when(outer)
    def _():
        for act, *where in (
            (near, 0), (own,), (near, 1), (relayx, 1), (near, 2), (near, 3), (fwd, 0), (relayy, 1), (far, 0),
            (far, 1), (far, 2), (diag, 1), (near, 4), (crossed, 1), (last, 0), (far, 3), (fwd, 1), (relayx, 2),
            (relayy, 2), (last, 1), (bwd, 1), (hand, 1), (crossed, 2), (relayx, 3), (diag, 2), (last, 2), (far, 4),
            (relayy, 3), (fwd, 2), (last, 3), (bwd, 2), (first, 2), (last, 4), (crossed, 3), (diag, 3), (firstB, 2),
            (bwd, 0), (second, 2), (fwd, 3), (first, 0), (bwd, 3), (tally,), (first, 3), (third, 2), (firstB, 3),
            (second, 3), (wg, 2), (firstB, 0), (third, 3), (second, 0), (wg, 3), (homeward,), (wg, 1), (third, 0),
        ):
            with jax.named_scope(act.__name__):
                act(*where)
        finish(nz - 1, (1, 2, 3))

    @pl.when(middle)
    def _():
        onto.update({2: behind, 3: ahead})
        for act, *where in (
            (last, 0), (near, 0), (own,), (near, 1), (pass_on, 0), (last, 1), (near, 2), (relayx, 1), (near, 3),
            (pass_on, 1), (relayy, 1), (relayx, 3), (pass_on, 2), (last, 2), (far, 0), (pass_on, 3), (relayy, 3),
            (last, 3), (far, 1), (near, 4), (diag, 1), (far, 2), (crossed, 1), (last, 4), (pass_on, 4), (far, 3),
            (fwd, 1), (bwd, 1), (hand, 1), (crossed, 3), (diag, 3), (far, 4), (fwd, 0), (relayx, 2), (relayy, 2),
            (fwd, 3), (bwd, 3), (first, 3), (crossed, 2), (diag, 2), (firstB, 3), (fwd, 2), (second, 3), (bwd, 2),
            (first, 2), (bwd, 0), (tally,), (third, 3), (firstB, 2), (second, 2), (first, 0), (firstB, 0), (wg, 2),
            (third, 2), (second, 0), (wg, 3), (homeward,), (wg, 1), (third, 0),
        ):
            with jax.named_scope(act.__name__):
                act(*where)
        finish(1, (2,))

    landed(home.at[pl.ds(0, ep - 1)], slot("home"))
    back_home = jnp.concatenate(
        [jnp.sum(jnp.where(named == e, home[j], 0.0), axis=0, keepdims=True) for j in range(ep)], axis=0)
    for k, hit in enumerate(hits):
        out_home[pl.ds(k, 1), :] = jnp.sum(jnp.where(hit, back_home, 0.0), axis=0, keepdims=True)
    assert sum(n for _, n in names.values()) == got.shape[0]
    drained("pair", other)
    drained("plane", full.at[pl.ds(0, 3), 0])
    drained("side", full.at[pl.ds(0, 4)])
    drained("own", full.at[0, 0, pl.ds(0, 3)])
    drained("hand", full.at[0, 0])
    drained("quarters", full.at[pl.ds(0, 7), 0, pl.ds(0, 2)])
    drained("home", weights.at[pl.ds(0, ep - 1)])
    drained("small", weights)

    @pl.when(middle)
    def _():
        drained("relay", full.at[pl.ds(0, 3), 0])
        drained("relay_w", weights.at[pl.ds(0, 4)])


def deliver(*refs):
    half = (len(refs) - 1) // 2
    copies = [pltpu.make_async_copy(src, dst, refs[-1].at[i])
              for i, (src, dst) in enumerate(zip(refs[:half], refs[half:-1]))]
    for copy in copies:
        copy.start()
    for copy in copies:
        copy.wait()


def dense(tokens, cotangent, routes, route_weight, w_gate, w_up, w_down):
    f32, bf16 = jnp.float32, jnp.bfloat16
    rows, width = tokens.shape
    ep, tp = lax.axis_size("ep"), lax.axis_size("tp")
    cols, half, nz, hidden = width // tp, rows // 2, ep // 2, w_gate.shape[2]
    anywhere, near = pl.BlockSpec(memory_space=pltpu.HBM), pl.BlockSpec(memory_space=pltpu.VMEM)

    def held(space, *arrays):
        return [pltpu.with_memory_space_constraint(x, space) for x in arrays]

    shapes = ((rows, cols), bf16), (routes.T.shape, f32), (w_gate.shape, f32), (w_up.shape, f32), (w_down.shape, f32)
    parts = pl.pallas_call(
        functools.partial(kernel, ep, tp),
        out_shape=tuple(pltpu.VMEM(*shape) for shape in shapes),
        in_specs=[anywhere] * 7,
        out_specs=(near,) * 5,
        scratch_shapes=[
            pltpu.VMEM((ep, 2, tp, rows, cols), bf16),
            pltpu.VMEM((width, 2 * hidden), bf16),
            pltpu.VMEM((hidden, width), bf16),
            pltpu.VMEM((ep, ep, rows), f32),
            pltpu.VMEM((ep, tp, rows, cols), bf16),
            pltpu.VMEM((nz, tp, rows, cols), bf16),
            pltpu.VMEM((nz, 4, half, cols), bf16),
            pltpu.VMEM((nz, 4, half, cols), bf16),
            pltpu.VMEM((nz, 2, half, cols), bf16),
            pltpu.VMEM((nz, 2, half, cols), bf16),
            pltpu.VMEM((nz, half, cols), bf16),
            pltpu.VMEM((nz, half, cols), bf16),
            pltpu.VMEM((2, rows, cols), bf16),
            pltpu.VMEM((nz, rows, cols), bf16),
            pltpu.VMEM((2, tp, rows, cols), bf16),
            pltpu.VMEM((ep, rows, 2 * hidden), bf16),
            pltpu.VMEM((ep, rows, hidden), bf16),
            pltpu.VMEM((ep, 8, rows), f32),
            pltpu.VMEM((ep, rows), f32),
            pltpu.VMEM((tp, ep, rows), f32),
            pltpu.VMEM((ep, rows), f32),
            pltpu.VMEM((ep, ep, rows), f32),
            pltpu.VMEM(routes.T.shape, routes.dtype),
            pltpu.VMEM(routes.T.shape, f32),
            pltpu.SemaphoreType.DMA((9,)),
            pltpu.SemaphoreType.DMA((10,)),
            pltpu.SemaphoreType.DMA((86,)),
        ],
        compiler_params=pltpu.CompilerParams(
            collective_id=0, has_side_effects=True, vmem_limit_bytes=50 * 1024 * 1024),
    )(*held(pltpu.HBM, tokens, cotangent, routes.T, route_weight.T, w_gate, w_up, w_down))
    grad_tokens, grw, *grads = pl.pallas_call(
        deliver,
        out_shape=tuple(jax.ShapeDtypeStruct(*shape) for shape in shapes),
        in_specs=[near] * 5,
        out_specs=(anywhere,) * 5,
        scratch_shapes=[pltpu.SemaphoreType.DMA((5,))],
        compiler_params=pltpu.CompilerParams(vmem_limit_bytes=1 << 20),
    )(*held(pltpu.VMEM, *parts))
    return grad_tokens, grw.T, *grads


def on_device(*args):
    rows, width = args[0].shape
    ep, tp = lax.axis_size("ep"), lax.axis_size("tp")
    fits = tp == 4 and ep == 8 and rows % 128 == 0 and 4 * rows * width * ep <= 1 << 24
    return (dense if fits else slotted)(*args)


def solution(mesh):
    return jax.shard_map(
        on_device,
        mesh=mesh,
        in_specs=(
            P("ep", None),
            P("ep", None),
            P("ep", None),
            P("ep", None),
            P("ep", None, "tp"),
            P("ep", None, "tp"),
            P("ep", "tp", None),
        ),
        out_specs=(
            P("ep", "tp"),
            P("ep", None),
            P("ep", None, "tp"),
            P("ep", None, "tp"),
            P("ep", "tp", None),
        ),
        check_vma=False,
    )
```
